128 devices in a mesh: sp: 32 (over z, y, core), tp: 4 (over x).
Axes of the slice: x: 4, y: 4, z: 4, core: 2. Of those that a mesh axis runs over, the one named last changes fastest.
Arguments:
- tokens: bfloat16 [4, 2048, 1024], P(None, 'sp', 'tp'), may hold values from -6 to 6
- norm_gain: float32 [4, 1024], replicated, may hold values from 0.1 to 1.9
- val_weight: bfloat16 [4, 1024, 512], P(None, 'sp', 'tp'), may hold values from -0.1875 to 0.1875
- gate_weight: bfloat16 [4, 1024, 512], P(None, 'sp', 'tp'), may hold values from -0.1875 to 0.1875
- conv_taps: float32 [4, 31, 512], P(None, None, 'tp'), may hold values from -1 to 1
- conv_bias: float32 [4, 512], P(None, 'tp'), may hold values from -3 to 3
- ln_gain: float32 [4, 512], P(None, 'tp'), may hold values from 0.1 to 1.9
- ln_shift: float32 [4, 512], P(None, 'tp'), may hold values from -3 to 3
- out_weight: bfloat16 [4, 512, 1024], P(None, 'tp', 'sp'), may hold values from -0.25 to 0.25
Outputs:
- stream: bfloat16 [4, 2048, 1024], P(None, 'sp', 'tp')
The draws below stay inside these ranges and needn't reach their ends.
All inputs are finite; a program needn't handle non-finite values.
Results may differ from the reference program's by a relative error of at most 0.02.
Values may be sent and summed in bfloat16 or wider, within the bound.
A program may use at most 64 MiB of HBM per device.

```python
import jax
import jax.numpy as jnp
from jax import lax

D = 1024
CHANNELS = 512
TAPS = 31
LAYERS = 4
SEQS = 4
TOKENS = 2048


def level_of(stream_key, dims, shards, low, top_value):
    level = 1.0
    for axis_at, shards_of in shards:
        heights = jax.random.uniform(jax.random.fold_in(jax.random.fold_in(stream_key, 6), axis_at), (shards_of,), jnp.float32, low / len(shards), top_value / len(shards))
        level = level * jnp.repeat(jnp.exp(heights), dims[axis_at] // shards_of).reshape((-1,) + (1,) * (len(dims) - 1 - axis_at))
    return level


def normal_values(own_key, shape, scale, most, shards=(), dtype=jnp.bfloat16):
    result = scale * jax.random.normal(own_key, shape, jnp.float32)
    if shards:
        result = result * level_of(own_key, shape, shards, -0.22, 0.18)
    return jnp.clip(result, -most, most).astype(dtype)


def setup_inputs(seed: int = 0) -> dict:
    splits = jax.random.split(jax.random.key(seed), 10)
    tokens = normal_values(splits[0], (SEQS, TOKENS, D), 1.0, 6.0, ((1, 32), (2, 4)))
    norm_gain = jnp.clip(1.0 + 0.18 * jax.random.normal(splits[1], (LAYERS, D), jnp.float32), 0.1, 1.9)
    val_weight = normal_values(splits[2], (LAYERS, D, CHANNELS), D ** -0.5, 0.1875, ((1, 32), (2, 4)))
    gate_weight = normal_values(splits[3], (LAYERS, D, CHANNELS), D ** -0.5, 0.1875, ((1, 32), (2, 4)))
    conv_taps = normal_values(splits[4], (LAYERS, TAPS, CHANNELS), TAPS ** -0.5, 1.0, ((2, 4),), jnp.float32)
    conv_bias = normal_values(splits[5], (LAYERS, CHANNELS), 0.5, 3.0, ((1, 4),), jnp.float32)
    ln_gain = jnp.clip(1.0 + 0.18 * jax.random.normal(splits[6], (LAYERS, CHANNELS), jnp.float32), 0.1, 1.9)
    ln_shift = normal_values(splits[7], (LAYERS, CHANNELS), 0.5, 3.0, ((1, 4),), jnp.float32)
    out_weight = normal_values(splits[8], (LAYERS, CHANNELS, D), CHANNELS ** -0.5, 0.25, ((1, 4), (2, 32)))
    return {"tokens": tokens, "norm_gain": norm_gain, "val_weight": val_weight, "gate_weight": gate_weight, "conv_taps": conv_taps, "conv_bias": conv_bias, "ln_gain": ln_gain, "ln_shift": ln_shift, "out_weight": out_weight}


epsilon = 1e-06

def depthwise(padded, tap_weights, length):
    running = padded[:, 0:length] * tap_weights[0]
    for tap_idx in range(1, tap_weights.shape[0]):
        running = running + padded[:, tap_idx:tap_idx + length] * tap_weights[tap_idx]
    return running

def reference(tokens, norm_gain, val_weight, gate_weight, conv_taps, conv_bias, ln_gain, ln_shift, out_weight):
    stream = tokens
    half_width = TAPS // 2
    for layer_idx in range(LAYERS):
        widened = stream.astype(jnp.float32)
        scaled = widened * jax.lax.rsqrt(lax.optimization_barrier(jnp.mean(widened * widened, axis=-1, keepdims=True)) + epsilon)
        normed = (scaled * norm_gain[layer_idx]).astype(jnp.bfloat16)
        tok_rows = normed.reshape(-1, D)
        values = jnp.dot(tok_rows, val_weight[layer_idx], preferred_element_type=jnp.float32)
        gates = jnp.dot(tok_rows, gate_weight[layer_idx], preferred_element_type=jnp.float32)
        gated = (values * jax.nn.sigmoid(gates)).astype(jnp.bfloat16).reshape(SEQS, TOKENS, CHANNELS)
        padded = jnp.pad(gated.astype(jnp.float32), ((0, 0), (half_width, half_width), (0, 0)))
        convolved = depthwise(padded, conv_taps[layer_idx], TOKENS) + conv_bias[layer_idx]
        mean_val = lax.optimization_barrier(jnp.mean(convolved, axis=-1, keepdims=True))
        centered = convolved - mean_val
        spread = lax.optimization_barrier(jnp.mean(centered * centered, axis=-1, keepdims=True))
        normalized = centered * jax.lax.rsqrt(spread + epsilon) * ln_gain[layer_idx] + ln_shift[layer_idx]
        activated = jax.nn.silu(normalized).astype(jnp.bfloat16).reshape(-1, CHANNELS)
        branch = jnp.dot(activated, out_weight[layer_idx], preferred_element_type=jnp.float32)
        stream = (stream.astype(jnp.float32) + branch.reshape(SEQS, TOKENS, D)).astype(jnp.bfloat16)
    return stream
```

```python
import jax
import jax.numpy as jnp
from jax import lax
from jax.sharding import PartitionSpec as P

LAYERS = 4
EPSILON = 1e-06
STEP = 16


def shards(
    tokens, norm_gain, val_weight, gate_weight, conv_taps, conv_bias, ln_gain, ln_shift, out_weight
):
    sp = lax.axis_index("sp")
    size = lax.axis_size("sp")
    length = tokens.shape[1]
    taps = conv_taps.shape[1]
    half = taps // 2
    own = lax.all_to_all(tokens, "tp", 0, 2, tiled=True)[0]
    up = [(i, (i + 1) % size) for i in range(size)]
    down = [(j, i) for i, j in up]
    before = lax.ppermute(own, "sp", up)
    after = lax.ppermute(own, "sp", down)
    stream = jnp.concatenate([before, own, after], axis=0)

    def whole(w, dim):
        w = lax.all_gather(w, "sp", axis=dim, tiled=True)
        return lax.all_gather(w, "tp", axis=3 - dim, tiled=True)

    small = lax.all_gather(
        jnp.concatenate([conv_taps, conv_bias[:, None], ln_gain[:, None], ln_shift[:, None]], axis=1),
        "tp", axis=2, tiled=True,
    )
    vals, gates, outs = whole(val_weight, 1), whole(gate_weight, 1), whole(out_weight, 2)
    position = sp * length - length + jnp.arange(3 * length)
    inside = (position >= 0) & (position < size * length)
    low = 0
    for layer in range(LAYERS):
        rows = stream.shape[0]
        widened = stream.astype(jnp.float32)
        scaled = widened * lax.rsqrt(jnp.mean(widened * widened, axis=-1, keepdims=True) + EPSILON)
        normed = (scaled * norm_gain[layer]).astype(jnp.bfloat16)
        values = jnp.dot(normed, vals[layer], preferred_element_type=jnp.float32)
        gate = jnp.dot(normed, gates[layer], preferred_element_type=jnp.float32)
        gated = (values * jax.nn.sigmoid(gate)).astype(jnp.bfloat16)
        gated = jnp.where(inside[low : low + rows, None], gated, 0).astype(jnp.float32)
        keep = rows - 2 * STEP
        first = STEP - half
        running = gated[first : first + keep] * small[layer, 0]
        for k in range(1, taps):
            running = running + gated[first + k : first + k + keep] * small[layer, k]
        convolved = running + small[layer, taps]
        mean = jnp.mean(convolved, axis=-1, keepdims=True)
        centered = convolved - mean
        spread = jnp.mean(centered * centered, axis=-1, keepdims=True)
        normalized = centered * lax.rsqrt(spread + EPSILON) * small[layer, taps + 1] + small[layer, taps + 2]
        activated = jax.nn.silu(normalized).astype(jnp.bfloat16)
        branch = jnp.dot(activated, outs[layer], preferred_element_type=jnp.float32)
        stream = (widened[STEP : STEP + keep] + branch).astype(jnp.bfloat16)
        low += STEP
    return lax.all_to_all(stream[None], "tp", 2, 0, tiled=True)


def solution(mesh):
    return jax.shard_map(
        shards,
        mesh=mesh,
        in_specs=(
            P(None, "sp", "tp"),
            P(),
            P(None, "sp", "tp"),
            P(None, "sp", "tp"),
            P(None, None, "tp"),
            P(None, "tp"),
            P(None, "tp"),
            P(None, "tp"),
            P(None, "tp", "sp"),
        ),
        out_specs=P(None, "sp", "tp"),
        check_vma=False,
    )
```

```python
import functools

import jax
import jax.numpy as jnp
from jax import lax
from jax.experimental import pallas as pl
from jax.experimental.pallas import tpu as pltpu
from jax.sharding import PartitionSpec as P

LAYERS = 4
EPSILON = 1e-06
STEP = 16
TAPS = 31
MESH = pl.DeviceIdType.MESH
F32, BF16 = jnp.float32, jnp.bfloat16
ORDERS = (("x", "y", "z"), ("y", "z", "x"), ("z", "x", "y"))
GROUPS = ((0, 1), (1, 3))
CHUNK = 32


def wrap(v, n):
    return lax.rem(v + n, n)


def kernel(
    tok, gain, val, gate, taps, bias, lng, lnb, outw, out,
    W, ow, ost, X, Y, N, V, G, GT, CV, A, O, gainv, T, S,
    loc, s1, r1, s2, r2, s3, r3, sd, rd, st, rt, sh, rh, sp_, rp_, so, ro,
):
    sp = lax.axis_index("sp")
    x = lax.axis_index("tp")
    n_sp = 32
    c = lax.rem(sp, 2)
    y = lax.rem(sp // 2, 4)
    z = sp // 8
    me = {"x": x, "y": y, "z": z}

    def device(d, step):
        at = dict(me)
        at[d] = wrap(me[d] + step, 4)
        return ((at["z"] * 4 + at["y"]) * 2 + c, at["x"])

    partner = (sp + 1 - 2 * c, x)
    left, right = (wrap(sp - 1, n_sp), x), (wrap(sp + 1, n_sp), x)
    across = (wrap(sp + 1 - 2 * (1 - c), n_sp), x)
    x_peers = [(sp, wrap(x + k, 4)) for k in (1, 2, 3)]

    cols = lambda i, w: pl.ds(pl.multiple_of(i * w, w), w)
    starts = [
        pltpu.make_async_copy(val, W.at[:, 0, z, y, c, :, cols(x, 128)], loc.at[0]),
        pltpu.make_async_copy(gate, W.at[:, 1, z, y, c, :, cols(x, 128)], loc.at[1]),
        pltpu.make_async_copy(outw, ow, loc.at[2]),
        pltpu.make_async_copy(tok.at[x], X.at[pl.ds(64, 64), cols(x, 256)], loc.at[3]),
        pltpu.make_async_copy(gain, gainv, loc.at[4]),
        pltpu.make_async_copy(taps, T.at[x], loc.at[5]),
        pltpu.make_async_copy(bias, S.at[x, 0], loc.at[6]),
        pltpu.make_async_copy(lng, S.at[x, 1], loc.at[7]),
        pltpu.make_async_copy(lnb, S.at[x, 2], loc.at[8]),
    ]
    for copy in starts:
        copy.start()

    barrier = pltpu.get_barrier_semaphore()
    peers = x_peers + [device("y", 1), device("y", -1), device("z", 1), device("z", -1), partner, across]
    for peer in peers:
        pl.semaphore_signal(barrier, inc=1, device_id=peer, device_id_type=MESH)

    starts[2].wait()
    eye = (
        lax.broadcasted_iota(jnp.int32, (32, 32), 0) == lax.broadcasted_iota(jnp.int32, (32, 32), 1)
    ).astype(BF16)
    for l in range(LAYERS):
        ost[l] = lax.dot_general(
            eye, ow[l], (((1,), (1,)), ((), ())), preferred_element_type=F32
        ).astype(BF16)
    place = pltpu.make_async_copy(ost, W.at[:, 2, z, y, c, :, cols(x, 128)], loc.at[9])
    place.start()
    starts[0].wait()
    starts[1].wait()
    pl.semaphore_wait(barrier, len(peers))

    sends = []

    def region(first, count, p, at, core, half):
        pick = lambda v: slice(None) if v is None else v
        rows = slice(None) if half is None else pl.ds(16 * half, 16)
        lanes = slice(None) if at["x"] is None else cols(at["x"], 128)
        return W.at[pl.ds(first, count), p, pick(at["z"]), pick(at["y"]), core, rows, lanes]

    def held(p, phase, coordinate):
        at = dict(me)
        for d in ORDERS[p][:phase]:
            at[d] = None
        at[ORDERS[p][phase]] = coordinate
        return at

    def remote(src, dst, ssem, rsem, to):
        return pltpu.make_async_remote_copy(
            src_ref=src, dst_ref=dst, send_sem=ssem, recv_sem=rsem, device_id=to, device_id_type=MESH
        )

    def ring(p, phase, first, count, ssem, rsem):
        d = ORDERS[p][phase]
        mine = me[d]

        def copy(kind):
            step = 1 if kind in (0, 2) else -1
            half = None if kind < 2 else kind - 2
            origin = mine if kind < 2 else wrap(mine - step, 4)
            part = region(first, count, p, held(p, phase, origin), c, half)
            return remote(part, part, ssem.at[kind], rsem.at[kind], device(d, step))

        def arrived(kind):
            step = 1 if kind in (0, 2) else -1
            half = None if kind < 2 else kind - 2
            origin = wrap(mine - step * (1 if kind < 2 else 2), 4)
            part = region(first, count, p, held(p, phase, origin), c, half)
            remote(part, part, ssem.at[kind], rsem.at[kind], device(d, step)).wait_recv()

        return copy, arrived

    def go(copy):
        copy.start()
        sends.append(copy)

    rings1 = [ring(p, 0, 0, LAYERS, s1.at[p], r1.at[p]) for p in range(3)]
    rings2 = [[ring(p, 1, f, n, s2.at[g, p], r2.at[g, p]) for p in range(3)] for g, (f, n) in enumerate(GROUPS)]
    rings3 = [[ring(p, 2, l, 1, s3.at[l, p], r3.at[l, p]) for p in range(3)] for l in range(LAYERS)]

    def send_full(rings):
        for kind in (0, 1):
            for copy, _ in rings:
                go(copy(kind))

    def forward(rings):
        for kind in (0, 1):
            for copy, arrived in rings:
                arrived(kind)
                go(copy(kind + 2))

    def finish(rings):
        for kind in (2, 3):
            for _, arrived in rings:
                arrived(kind)

    for kind in (0, 1):
        for p in (0, 1):
            go(rings1[p][0](kind))
    place.wait()
    for kind in (0, 1):
        go(rings1[2][0](kind))
    for k, to in enumerate(x_peers):
        go(remote(tok.at[to[1]], X.at[pl.ds(64, 64), cols(x, 256)], st.at[k], rt.at[k], to))
    forward(rings1)
    for k, to in enumerate(x_peers):
        go(remote(taps, T.at[x], sp_.at[k, 0], rp_.at[k, 0], to))
        go(remote(bias, S.at[x, 0], sp_.at[k, 1], rp_.at[k, 1], to))
        go(remote(lng, S.at[x, 1], sp_.at[k, 2], rp_.at[k, 2], to))
        go(remote(lnb, S.at[x, 2], sp_.at[k, 3], rp_.at[k, 3], to))
    finish(rings1)

    send_full(rings2[0])
    starts[3].wait()
    for k in range(3):
        origin = wrap(x - (k + 1), 4)
        part = X.at[pl.ds(64, 64), cols(origin, 256)]
        remote(part, part, st.at[k], rt.at[k], x_peers[k]).wait_recv()
    core_rows = X.at[pl.ds(64, 64)]
    go(remote(core_rows, X.at[pl.ds(0, 64)], sh.at[0], rh.at[0], right))
    go(remote(core_rows, X.at[pl.ds(128, 64)], sh.at[1], rh.at[1], left))
    send_full(rings2[1])
    forward(rings2[0])

    def hand(l, p, kind):
        step, half = ((0, None), (1, None), (-1, None), (2, 0), (2, 1))[kind]
        at = held(p, 2, wrap(me[ORDERS[p][2]] - step, 4))
        part = region(l, 1, p, at, c, half)
        go(remote(part, part, sd.at[l, p, kind], rd.at[l, p, kind], partner))

    def handed(l):
        for kind, (step, half) in enumerate(((0, None), (1, None), (-1, None), (2, 0), (2, 1))):
            for p in range(3):
                at = held(p, 2, wrap(me[ORDERS[p][2]] - step, 4))
                part = region(l, 1, p, at, 1 - c, half)
                remote(part, part, sd.at[l, p, kind], rd.at[l, p, kind], partner).wait_recv()

    def full3(l):
        send_full(rings3[l])
        for p in range(3):
            hand(l, p, 0)

    def forward3(l):
        for kind in (0, 1):
            for p, (copy, arrived) in enumerate(rings3[l]):
                arrived(kind)
                go(copy(kind + 2))
                hand(l, p, kind + 1)

    def finish3(l):
        for kind in (2, 3):
            for p, (_, arrived) in enumerate(rings3[l]):
                arrived(kind)
                hand(l, p, kind + 1)

    finish(rings2[0])
    full3(0)
    forward(rings2[1])
    finish(rings2[1])
    full3(1)
    forward3(0)
    full3(2)

    for k in range(4, 9):
        starts[k].wait()
    for k in range(3):
        origin = wrap(x - (k + 1), 4)
        for j, part in enumerate((T.at[origin], S.at[origin, 0], S.at[origin, 1], S.at[origin, 2])):
            remote(part, part, sp_.at[k, j], rp_.at[k, j], x_peers[k]).wait_recv()
    for k, rows in enumerate((0, 128)):
        part = X.at[pl.ds(rows, 64)]
        remote(core_rows, part, sh.at[k], rh.at[k], (right, left)[k]).wait_recv()

    def norm(l):
        low, rows = STEP * l, 192 - 2 * STEP * l
        src = X if l == 0 else Y
        g = gainv[l : l + 1, :]

        @pl.loop(0, rows // 16)
        def _(i):
            r = pl.multiple_of(low + i * 16, 16)
            v = src[pl.ds(r, 16), :].astype(F32)
            scaled = v * lax.rsqrt(jnp.mean(v * v, axis=-1, keepdims=True) + EPSILON)
            N[pl.ds(r, 16), :] = (scaled * g).astype(BF16)

    def project(l, p, dst):
        low, rows = STEP * l, 192 - 2 * STEP * l
        w = W[l, p].reshape(1024, 512)
        dst[pl.ds(low, rows), :] = jnp.dot(N[pl.ds(low, rows), :], w, preferred_element_type=F32)

    def gating(l):
        low, rows = STEP * l, 192 - 2 * STEP * l

        @pl.loop(0, rows // 16)
        def _(i):
            r = pl.multiple_of(low + i * 16, 16)
            at = pl.ds(r, 16)
            g = (V[at, :] * jax.nn.sigmoid(G[at, :])).astype(BF16).astype(F32)
            where = sp * 64 - 64 + r + lax.broadcasted_iota(jnp.int32, (16, 512), 0)
            g = jnp.where((where >= 0) & (where < 2048), g, 0.0)
            for j in range(4):
                GT[j, at, :] = g[:, 128 * j : 128 * j + 128]

    def conv(l):
        low, rows = STEP * (l + 1), 192 - 2 * STEP * (l + 1)
        for j in range(4):
            for r in range(low, low + rows, CHUNK):
                acc = jnp.zeros((CHUNK, 128), F32) + S[j, 0, l : l + 1, :]
                for k in range(TAPS):
                    acc = acc + GT[j, r + k - 15 : r + k - 15 + CHUNK, :] * T[j, l, k : k + 1, :]
                CV[r : r + CHUNK, 128 * j : 128 * j + 128] = acc

    def channel_norm(l):
        low, rows = STEP * (l + 1), 192 - 2 * STEP * (l + 1)
        g = jnp.concatenate([S[j, 1, l : l + 1, :] for j in range(4)], axis=1)
        b = jnp.concatenate([S[j, 2, l : l + 1, :] for j in range(4)], axis=1)

        @pl.loop(0, rows // 16)
        def _(i):
            at = pl.ds(pl.multiple_of(low + i * 16, 16), 16)
            v = CV[at, :]
            centered = v - jnp.mean(v, axis=-1, keepdims=True)
            spread = jnp.mean(centered * centered, axis=-1, keepdims=True)
            v = centered * lax.rsqrt(spread + EPSILON) * g + b
            A[at, :] = (v * jax.nn.sigmoid(v)).astype(BF16)

    def output(l):
        low, rows = STEP * (l + 1), 192 - 2 * STEP * (l + 1)
        src = X if l == 0 else Y
        for q in range(4):
            w = W[l, 2, q].reshape(256, 512)
            branch = lax.dot_general(
                A[pl.ds(low, rows), :], w, (((1,), (1,)), ((), ())), preferred_element_type=F32
            )
            lanes = slice(256 * q, 256 * q + 256)
            total = (src[low : low + rows, lanes].astype(F32) + branch).astype(BF16)
            if l + 1 < LAYERS:
                Y[low : low + rows, lanes] = total
            else:
                O[q] = total

    def compute(l, between=()):
        steps = [
            functools.partial(norm, l),
            functools.partial(project, l, 0, V),
            functools.partial(project, l, 1, G),
            functools.partial(gating, l),
            functools.partial(conv, l),
            functools.partial(channel_norm, l),
            functools.partial(output, l),
        ]
        between = dict(between)
        for i, step in enumerate(steps):
            if i in between:
                between[i]()
            step()

    forward3(1)
    finish3(0)
    full3(3)
    handed(0)
    compute(0, {3: lambda: forward3(2), 5: lambda: finish3(1)})
    handed(1)
    compute(1, {3: lambda: forward3(3), 5: lambda: finish3(2)})
    handed(2)
    compute(2, {5: lambda: finish3(3)})
    handed(3)
    compute(3)

    mine = pltpu.make_async_copy(O.at[x], out.at[x], loc.at[10])
    mine.start()
    for k, to in enumerate(x_peers):
        go(remote(O.at[to[1]], out.at[x], so.at[k], ro.at[k], to))
    for k in range(3):
        part = out.at[wrap(x - (k + 1), 4)]
        remote(O.at[0], part, so.at[k], ro.at[k], x_peers[k]).wait_recv()
    mine.wait()
    for copy in sends:
        copy.wait_send()


def shards(tokens, norm_gain, val_weight, gate_weight, conv_taps, conv_bias, ln_gain, ln_shift, out_weight):
    any_ = pl.BlockSpec(memory_space=pl.ANY)
    dma = pltpu.SemaphoreType.DMA
    vmem = pltpu.VMEM
    return pl.pallas_call(
        kernel,
        name="conv_stack",
        out_shape=jax.ShapeDtypeStruct(tokens.shape, tokens.dtype),
        in_specs=[any_] * 9,
        out_specs=any_,
        scratch_shapes=[
            vmem((LAYERS, 3, 4, 4, 2, 32, 512), BF16),
            vmem((LAYERS, 128, 32), BF16),
            vmem((LAYERS, 32, 128), BF16),
            vmem((192, 1024), BF16),
            vmem((192, 1024), BF16),
            vmem((192, 1024), BF16),
            vmem((192, 512), F32),
            vmem((192, 512), F32),
            vmem((4, 192, 128), F32),
            vmem((192, 512), F32),
            vmem((192, 512), BF16),
            vmem((4, 64, 256), BF16),
            vmem((LAYERS, 1024), F32),
            vmem((4, LAYERS, TAPS, 128), F32),
            vmem((4, 3, LAYERS, 128), F32),
            dma((11,)),
            dma((3, 4)), dma((3, 4)),
            dma((2, 3, 4)), dma((2, 3, 4)),
            dma((LAYERS, 3, 4)), dma((LAYERS, 3, 4)),
            dma((LAYERS, 3, 5)), dma((LAYERS, 3, 5)),
            dma((3,)), dma((3,)),
            dma((2,)), dma((2,)),
            dma((3, 4)), dma((3, 4)),
            dma((3,)), dma((3,)),
        ],
        compiler_params=pltpu.CompilerParams(
            collective_id=0, has_side_effects=True, vmem_limit_bytes=40 * 1024 * 1024
        ),
    )(tokens, norm_gain, val_weight, gate_weight, conv_taps, conv_bias, ln_gain, ln_shift, out_weight)


def solution(mesh):
    return jax.shard_map(
        shards,
        mesh=mesh,
        in_specs=(
            P(None, "sp", "tp"),
            P(),
            P(None, "sp", "tp"),
            P(None, "sp", "tp"),
            P(None, None, "tp"),
            P(None, "tp"),
            P(None, "tp"),
            P(None, "tp"),
            P(None, "tp", "sp"),
        ),
        out_specs=P(None, "sp", "tp"),
        check_vma=False,
    )
```

```python
import functools

import jax
import jax.numpy as jnp
from jax import lax
from jax.experimental import pallas as pl
from jax.experimental.pallas import tpu as pltpu
from jax.sharding import PartitionSpec as P

LAYERS = 4
EPSILON = 1e-06
STEP = 16
TAPS = 31
MESH = pl.DeviceIdType.MESH
F32, BF16 = jnp.float32, jnp.bfloat16
ORDERS = (("x", "y", "z"), ("y", "z", "x"), ("z", "x", "y"))
GROUPS = ((0, 1), (1, 3))
CHUNK = 32


def wrap(v, n):
    return lax.rem(v + n, n)


def kernel(
    tok, gain, val, gate, taps, bias, lng, lnb, outw, out,
    W, X, Y, N, V, G, GT, CV, A, O, gainv, T,
    loc, s1, r1, s2, r2, s3, r3, sd, rd, st, rt, sh, rh, sp_, rp_, so, ro,
):
    sp = lax.axis_index("sp")
    x = lax.axis_index("tp")
    n_sp = 32
    c = lax.rem(sp, 2)
    y = lax.rem(sp // 2, 4)
    z = sp // 8
    me = {"x": x, "y": y, "z": z}

    def device(d, step):
        at = dict(me)
        at[d] = wrap(me[d] + step, 4)
        return ((at["z"] * 4 + at["y"]) * 2 + c, at["x"])

    partner = (sp + 1 - 2 * c, x)
    across = (wrap(sp + 1 - 2 * (1 - c), n_sp), x)
    x_peers = [(sp, wrap(x + k, 4)) for k in (1, 2, 3)]

    barrier = pltpu.get_barrier_semaphore()
    peers = [device(d, step) for d in "xyz" for step in (1, -1)] + [partner]
    for peer in peers:
        pl.semaphore_signal(barrier, inc=1, device_id=peer, device_id_type=MESH)

    cols = lambda i, w: pl.ds(pl.multiple_of(i * w, w), w)
    parts = (val, gate, outw)
    starts = [pltpu.make_async_copy(w, W.at[:, p, z, y, c, :, cols(x, 128)], loc.at[p]) for p, w in enumerate(parts)]
    starts += [
        pltpu.make_async_copy(tok.at[x], X.at[pl.ds(64, 64), cols(x, 256)], loc.at[3]),
        pltpu.make_async_copy(gain, gainv, loc.at[4]),
        pltpu.make_async_copy(taps, T.at[x, pl.ds(0, TAPS)], loc.at[5]),
        pltpu.make_async_copy(bias, T.at[x, TAPS], loc.at[6]),
        pltpu.make_async_copy(lng, T.at[x, TAPS + 1], loc.at[7]),
        pltpu.make_async_copy(lnb, T.at[x, TAPS + 2], loc.at[8]),
    ]
    for copy in starts:
        copy.start()
    for copy in starts:
        copy.wait()
    pl.semaphore_wait(barrier, len(peers))

    sends = []

    def region(first, count, p, at, core, half):
        pick = lambda v: slice(None) if v is None else v
        rows = slice(None) if half is None else pl.ds(16 * half, 16)
        lanes = slice(None) if at["x"] is None else cols(at["x"], 128)
        return W.at[pl.ds(first, count), p, pick(at["z"]), pick(at["y"]), core, rows, lanes]

    def held(p, phase, coordinate):
        at = dict(me)
        for d in ORDERS[p][:phase]:
            at[d] = None
        at[ORDERS[p][phase]] = coordinate
        return at

    def remote(src, dst, ssem, rsem, to):
        return pltpu.make_async_remote_copy(
            src_ref=src, dst_ref=dst, send_sem=ssem, recv_sem=rsem, device_id=to, device_id_type=MESH
        )

    def ring(p, phase, first, count, ssem, rsem):
        d = ORDERS[p][phase]
        mine = me[d]

        def copy(kind):
            step = 1 if kind in (0, 2) else -1
            half = None if kind < 2 else kind - 2
            origin = mine if kind < 2 else wrap(mine - step, 4)
            part = region(first, count, p, held(p, phase, origin), c, half)
            return remote(part, part, ssem.at[kind], rsem.at[kind], device(d, step))

        def arrived(kind):
            step = 1 if kind in (0, 2) else -1
            half = None if kind < 2 else kind - 2
            origin = wrap(mine - step * (1 if kind < 2 else 2), 4)
            part = region(first, count, p, held(p, phase, origin), c, half)
            remote(part, part, ssem.at[kind], rsem.at[kind], device(d, step)).wait_recv()

        return copy, arrived

    def go(copy):
        copy.start()
        sends.append(copy)

    rings1 = [ring(p, 0, 0, LAYERS, s1.at[p], r1.at[p]) for p in range(3)]
    rings2 = [[ring(p, 1, f, n, s2.at[g, p], r2.at[g, p]) for p in range(3)] for g, (f, n) in enumerate(GROUPS)]
    rings3 = [[ring(p, 2, l, 1, s3.at[l, p], r3.at[l, p]) for p in range(3)] for l in range(LAYERS)]

    def send_full(rings):
        for kind in (0, 1):
            for copy, _ in rings:
                go(copy(kind))

    def forward(rings):
        for kind in (0, 1):
            for copy, arrived in rings:
                arrived(kind)
                go(copy(kind + 2))

    def finish(rings):
        for kind in (2, 3):
            for _, arrived in rings:
                arrived(kind)

    send_full(rings1)

    def send_tokens(k):
        go(remote(tok.at[x_peers[k][1]], X.at[pl.ds(64, 64), cols(x, 256)], st.at[k], rt.at[k], x_peers[k]))

    share = pl.ds(17 * c, 17)

    def send_parameters(k):
        go(remote(T.at[x, share], T.at[x, share], sp_.at[0, k], rp_.at[0, k], x_peers[k]))

    for k in (0, 2):
        send_tokens(k)
    for k in (0, 2):
        send_parameters(k)
    forward(rings1)
    finish(rings1)

    send_full(rings2[0])
    send_tokens(1)
    send_parameters(1)
    send_full(rings2[1])
    forward(rings2[0])
    for k in range(3):
        part = X.at[pl.ds(64, 64), cols(wrap(x - (k + 1), 4), 256)]
        remote(part, part, st.at[k], rt.at[k], x_peers[k]).wait_recv()
    core_rows = X.at[pl.ds(64, 64)]
    near = X.at[pl.ds(128 * c, 64)]
    far = X.at[pl.ds(128 - 128 * c, 64)]
    go(remote(core_rows, near, sh.at[0], rh.at[0], partner))

    def hand(l, p, kind):
        step, half = ((0, None), (1, None), (-1, None), (2, 0), (2, 1))[kind]
        at = held(p, 2, wrap(me[ORDERS[p][2]] - step, 4))
        part = region(l, 1, p, at, c, half)
        go(remote(part, part, sd.at[l, p, kind], rd.at[l, p, kind], partner))

    def handed(l, kinds=(0, 1, 2, 3, 4)):
        for kind in kinds:
            step, half = ((0, None), (1, None), (-1, None), (2, 0), (2, 1))[kind]
            for p in range(3):
                at = held(p, 2, wrap(me[ORDERS[p][2]] - step, 4))
                part = region(l, 1, p, at, 1 - c, half)
                remote(part, part, sd.at[l, p, kind], rd.at[l, p, kind], partner).wait_recv()

    def full3(l):
        send_full(rings3[l])
        for p in range(3):
            hand(l, p, 0)

    def forward3(l):
        for kind in (0, 1):
            for p, (copy, arrived) in enumerate(rings3[l]):
                arrived(kind)
                go(copy(kind + 2))
                hand(l, p, kind + 1)

    def finish3(l):
        for kind in (2, 3):
            for p, (_, arrived) in enumerate(rings3[l]):
                arrived(kind)
                hand(l, p, kind + 1)

    finish(rings2[0])
    full3(0)
    handed(0, (0,))
    go(remote(core_rows, far, sh.at[1], rh.at[1], across))
    forward(rings2[1])
    finish(rings2[1])
    full3(1)
    forward3(0)
    full3(2)

    for k in range(3):
        origin = wrap(x - (k + 1), 4)
        part = T.at[origin, share]
        remote(part, part, sp_.at[0, k], rp_.at[0, k], x_peers[k]).wait_recv()
        go(remote(part, part, sp_.at[1, k], rp_.at[1, k], partner))

    def norm(l):
        low, rows = STEP * l, 192 - 2 * STEP * l
        src = X if l == 0 else Y
        g = gainv[l : l + 1, :]

        @pl.loop(0, rows // 16)
        def _(i):
            r = pl.multiple_of(low + i * 16, 16)
            v = src[pl.ds(r, 16), :].astype(F32)
            scaled = v * lax.rsqrt(jnp.mean(v * v, axis=-1, keepdims=True) + EPSILON)
            N[pl.ds(r, 16), :] = (scaled * g).astype(BF16)

    def project(l, p, dst):
        low, rows = STEP * l, 192 - 2 * STEP * l
        w = W[l, p].reshape(1024, 512)
        dst[pl.ds(low, rows), :] = jnp.dot(N[pl.ds(low, rows), :], w, preferred_element_type=F32)

    def gating(l):
        low, rows = STEP * l, 192 - 2 * STEP * l

        @pl.loop(0, rows // 16)
        def _(i):
            r = pl.multiple_of(low + i * 16, 16)
            at = pl.ds(r, 16)
            g = (V[at, :] * jax.nn.sigmoid(G[at, :])).astype(BF16).astype(F32)
            where = sp * 64 - 64 + r + lax.broadcasted_iota(jnp.int32, (16, 512), 0)
            g = jnp.where((where >= 0) & (where < 2048), g, 0.0)
            for j in range(4):
                GT[j, at, :] = g[:, 128 * j : 128 * j + 128]

    def conv(l):
        low, rows = STEP * (l + 1), 192 - 2 * STEP * (l + 1)
        for j in range(4):
            for r in range(low, low + rows, CHUNK):
                acc = jnp.zeros((CHUNK, 128), F32) + T[j, TAPS, l : l + 1, :]
                for k in range(TAPS):
                    acc = acc + GT[j, r + k - 15 : r + k - 15 + CHUNK, :] * T[j, k, l : l + 1, :]
                CV[r : r + CHUNK, 128 * j : 128 * j + 128] = acc

    def channel_norm(l):
        low, rows = STEP * (l + 1), 192 - 2 * STEP * (l + 1)
        g = jnp.concatenate([T[j, TAPS + 1, l : l + 1, :] for j in range(4)], axis=1)
        b = jnp.concatenate([T[j, TAPS + 2, l : l + 1, :] for j in range(4)], axis=1)

        @pl.loop(0, rows // 16)
        def _(i):
            at = pl.ds(pl.multiple_of(low + i * 16, 16), 16)
            v = CV[at, :]
            centered = v - jnp.mean(v, axis=-1, keepdims=True)
            spread = jnp.mean(centered * centered, axis=-1, keepdims=True)
            v = centered * lax.rsqrt(spread + EPSILON) * g + b
            A[at, :] = (v * jax.nn.sigmoid(v)).astype(BF16)

    def output(l):
        low, rows = STEP * (l + 1), 192 - 2 * STEP * (l + 1)
        src = X if l == 0 else Y
        for q in range(4):
            w = W[l, 2, q].reshape(256, 512)
            branch = lax.dot_general(
                A[pl.ds(low, rows), :], w, (((1,), (1,)), ((), ())), preferred_element_type=F32
            )
            lanes = slice(256 * q, 256 * q + 256)
            total = (src[low : low + rows, lanes].astype(F32) + branch).astype(BF16)
            if l + 1 < LAYERS:
                Y[low : low + rows, lanes] = total
            else:
                O[q] = total

    def compute(l, between=()):
        steps = [
            functools.partial(norm, l),
            functools.partial(project, l, 0, V),
            functools.partial(project, l, 1, G),
            functools.partial(gating, l),
            functools.partial(conv, l),
            functools.partial(channel_norm, l),
            functools.partial(output, l),
        ]
        between = dict(between)
        for i, step in enumerate(steps):
            if i in between:
                between[i]()
            step()

    forward3(1)
    finish3(0)
    full3(3)
    handed(0, (1, 2, 3, 4))
    for k in range(3):
        origin = wrap(x - (k + 1), 4)
        part = T.at[origin, pl.ds(17 - 17 * c, 17)]
        remote(part, part, sp_.at[1, k], rp_.at[1, k], partner).wait_recv()
    remote(core_rows, far, sh.at[0], rh.at[0], partner).wait_recv()
    remote(core_rows, near, sh.at[1], rh.at[1], across).wait_recv()
    compute(0, {3: lambda: forward3(2), 5: lambda: finish3(1)})
    handed(1)
    compute(1, {3: lambda: forward3(3), 5: lambda: finish3(2)})
    handed(2)
    compute(2, {5: lambda: finish3(3)})
    handed(3)
    compute(3)

    mine = pltpu.make_async_copy(O.at[x], out.at[x], loc.at[10])
    mine.start()
    for k, to in enumerate(x_peers):
        go(remote(O.at[to[1]], out.at[x], so.at[k], ro.at[k], to))
    for k in range(3):
        part = out.at[wrap(x - (k + 1), 4)]
        remote(O.at[0], part, so.at[k], ro.at[k], x_peers[k]).wait_recv()
    mine.wait()
    for copy in sends:
        copy.wait_send()


def shards(tokens, norm_gain, val_weight, gate_weight, conv_taps, conv_bias, ln_gain, ln_shift, out_weight):
    any_ = pl.BlockSpec(memory_space=pl.ANY)
    dma = pltpu.SemaphoreType.DMA
    vmem = pltpu.VMEM
    return pl.pallas_call(
        kernel,
        name="conv_stack",
        out_shape=jax.ShapeDtypeStruct(tokens.shape, tokens.dtype),
        in_specs=[any_] * 9,
        out_specs=any_,
        scratch_shapes=[
            vmem((LAYERS, 3, 4, 4, 2, 32, 512), BF16),
            vmem((192, 1024), BF16),
            vmem((192, 1024), BF16),
            vmem((192, 1024), BF16),
            vmem((192, 512), F32),
            vmem((192, 512), F32),
            vmem((4, 192, 128), F32),
            vmem((192, 512), F32),
            vmem((192, 512), BF16),
            vmem((4, 64, 256), BF16),
            vmem((LAYERS, 1024), F32),
            vmem((4, TAPS + 3, LAYERS, 128), F32),
            dma((11,)),
            dma((3, 4)), dma((3, 4)),
            dma((2, 3, 4)), dma((2, 3, 4)),
            dma((LAYERS, 3, 4)), dma((LAYERS, 3, 4)),
            dma((LAYERS, 3, 5)), dma((LAYERS, 3, 5)),
            dma((3,)), dma((3,)),
            dma((2,)), dma((2,)),
            dma((2, 3)), dma((2, 3)),
            dma((3,)), dma((3,)),
        ],
        compiler_params=pltpu.CompilerParams(
            collective_id=0, has_side_effects=True, vmem_limit_bytes=40 * 1024 * 1024
        ),
    )(
        tokens, norm_gain, val_weight, gate_weight, conv_taps.transpose(1, 0, 2), conv_bias, ln_gain, ln_shift,
        out_weight.transpose(0, 2, 1),
    )


def solution(mesh):
    return jax.shard_map(
        shards,
        mesh=mesh,
        in_specs=(
            P(None, "sp", "tp"),
            P(),
            P(None, "sp", "tp"),
            P(None, "sp", "tp"),
            P(None, None, "tp"),
            P(None, "tp"),
            P(None, "tp"),
            P(None, "tp"),
            P(None, "tp", "sp"),
        ),
        out_specs=P(None, "sp", "tp"),
        check_vma=False,
    )
```

```python
import functools

import jax
import jax.numpy as jnp
from jax import lax
from jax.experimental import pallas as pl
from jax.experimental.pallas import tpu as pltpu
from jax.sharding import PartitionSpec as P

LAYERS = 4
EPSILON = 1e-06
STEP = 16
TAPS = 31
MESH = pl.DeviceIdType.MESH
F32, BF16 = jnp.float32, jnp.bfloat16
ORDERS = (("x", "y", "z"), ("y", "z", "x"), ("z", "x", "y"))
GROUPS = ((0, 1), (1, 3))
CHUNK = 32


def wrap(v, n):
    return lax.rem(v + n, n)


def kernel(
    tok, gain, val, gate, taps, bias, lng, lnb, outw, out,
    W, X, Y, N, V, G, GT, CV, A, O, gainv, T,
    loc, s1, r1, s2, r2, s3, r3, sd, rd, st, rt, sh, rh, sp_, rp_, so, ro,
):
    sp = lax.axis_index("sp")
    x = lax.axis_index("tp")
    n_sp = 32
    c = lax.rem(sp, 2)
    y = lax.rem(sp // 2, 4)
    z = sp // 8
    me = {"x": x, "y": y, "z": z}

    def device(d, step):
        at = dict(me)
        at[d] = wrap(me[d] + step, 4)
        return ((at["z"] * 4 + at["y"]) * 2 + c, at["x"])

    partner = (sp + 1 - 2 * c, x)
    across = (wrap(sp + 1 - 2 * (1 - c), n_sp), x)
    x_peers = [(sp, wrap(x + k, 4)) for k in (1, 2, 3)]

    barrier = pltpu.get_barrier_semaphore()
    peers = [device(d, step) for d in "xyz" for step in (1, 2, 3)] + [partner]
    for peer in peers:
        pl.semaphore_signal(barrier, inc=1, device_id=peer, device_id_type=MESH)

    cols = lambda i, w: pl.ds(pl.multiple_of(i * w, w), w)
    parts = (val, gate, outw)
    starts = [pltpu.make_async_copy(w, W.at[:, p, z, y, c, :, cols(x, 128)], loc.at[p]) for p, w in enumerate(parts)]
    starts += [
        pltpu.make_async_copy(tok.at[x], X.at[pl.ds(64, 64), cols(x, 256)], loc.at[3]),
        pltpu.make_async_copy(gain, gainv, loc.at[4]),
        pltpu.make_async_copy(taps, T.at[x, pl.ds(0, TAPS)], loc.at[5]),
        pltpu.make_async_copy(bias, T.at[x, TAPS], loc.at[6]),
        pltpu.make_async_copy(lng, T.at[x, TAPS + 1], loc.at[7]),
        pltpu.make_async_copy(lnb, T.at[x, TAPS + 2], loc.at[8]),
    ]
    for copy in starts:
        copy.start()
    for copy in starts:
        copy.wait()
    pl.semaphore_wait(barrier, len(peers))

    sends = []

    def region(first, count, p, at, core, half):
        pick = lambda v: slice(None) if v is None else v
        rows = slice(None) if half is None else pl.ds(16 * half, 16)
        lanes = slice(None) if at["x"] is None else cols(at["x"], 128)
        return W.at[pl.ds(first, count), p, pick(at["z"]), pick(at["y"]), core, rows, lanes]

    def held(p, phase, coordinate):
        at = dict(me)
        for d in ORDERS[p][:phase]:
            at[d] = None
        at[ORDERS[p][phase]] = coordinate
        return at

    def remote(src, dst, ssem, rsem, to):
        return pltpu.make_async_remote_copy(
            src_ref=src, dst_ref=dst, send_sem=ssem, recv_sem=rsem, device_id=to, device_id_type=MESH
        )

    def ring(p, phase, first, count, ssem, rsem):
        d = ORDERS[p][phase]
        mine = me[d]

        def copy(kind):
            step = 1 if kind in (0, 2) else -1
            half = None if kind < 2 else kind - 2
            origin = mine if kind < 2 else wrap(mine - step, 4)
            part = region(first, count, p, held(p, phase, origin), c, half)
            return remote(part, part, ssem.at[kind], rsem.at[kind], device(d, step))

        def arrived(kind):
            step = 1 if kind in (0, 2) else -1
            half = None if kind < 2 else kind - 2
            origin = wrap(mine - step * (1 if kind < 2 else 2), 4)
            part = region(first, count, p, held(p, phase, origin), c, half)
            remote(part, part, ssem.at[kind], rsem.at[kind], device(d, step)).wait_recv()

        return copy, arrived

    def go(copy):
        copy.start()
        sends.append(copy)

    def spread(p, phase, first, count, ssem, rsem):
        d = ORDERS[p][phase]

        def copy(k):
            part = region(first, count, p, held(p, phase, me[d]), c, None)
            return remote(part, part, ssem.at[k - 1], rsem.at[k - 1], device(d, k))

        def arrived(k):
            part = region(first, count, p, held(p, phase, wrap(me[d] - k, 4)), c, None)
            remote(part, part, ssem.at[k - 1], rsem.at[k - 1], device(d, k)).wait_recv()

        return copy, arrived

    spreads1 = [[spread(p, 0, f, n, s1.at[g, p], r1.at[g, p]) for p in range(3)] for g, (f, n) in enumerate(GROUPS)]
    spreads2 = [[spread(p, 1, f, n, s2.at[g, p], r2.at[g, p]) for p in range(3)] for g, (f, n) in enumerate(GROUPS)]
    rings3 = [[ring(p, 2, l, 1, s3.at[l, p], r3.at[l, p]) for p in range(3)] for l in range(LAYERS)]

    def send_spread(spreads):
        for k in (2, 1, 3):
            for copy, _ in spreads:
                go(copy(k))

    def end_spread(spreads):
        for k in (1, 3, 2):
            for _, arrived in spreads:
                arrived(k)

    def send_full(rings):
        for kind in (0, 1):
            for copy, _ in rings:
                go(copy(kind))

    def send_tokens(k):
        go(remote(tok.at[x_peers[k][1]], X.at[pl.ds(64, 64), cols(x, 256)], st.at[k], rt.at[k], x_peers[k]))

    share = pl.ds(17 * c, 17)

    def send_parameters(k):
        go(remote(T.at[x, share], T.at[x, share], sp_.at[0, k], rp_.at[0, k], x_peers[k]))

    send_spread(spreads1[0])
    send_spread(spreads1[1])
    for k in (1, 0, 2):
        send_tokens(k)
    end_spread(spreads1[0])
    send_spread(spreads2[0])
    end_spread(spreads1[1])
    send_spread(spreads2[1])
    for k in (1, 0, 2):
        send_parameters(k)
    for k in range(3):
        part = X.at[pl.ds(64, 64), cols(wrap(x - (k + 1), 4), 256)]
        remote(part, part, st.at[k], rt.at[k], x_peers[k]).wait_recv()
    core_rows = X.at[pl.ds(64, 64)]
    near = X.at[pl.ds(128 * c, 64)]
    far = X.at[pl.ds(128 - 128 * c, 64)]
    go(remote(core_rows, near, sh.at[0], rh.at[0], partner))

    def hand(l, p, kind):
        step, half = ((0, None), (1, None), (-1, None), (2, 0), (2, 1))[kind]
        at = held(p, 2, wrap(me[ORDERS[p][2]] - step, 4))
        part = region(l, 1, p, at, c, half)
        go(remote(part, part, sd.at[l, p, kind], rd.at[l, p, kind], partner))

    def handed(l, kinds=(0, 1, 2, 3, 4)):
        for kind in kinds:
            step, half = ((0, None), (1, None), (-1, None), (2, 0), (2, 1))[kind]
            for p in range(3):
                at = held(p, 2, wrap(me[ORDERS[p][2]] - step, 4))
                part = region(l, 1, p, at, 1 - c, half)
                remote(part, part, sd.at[l, p, kind], rd.at[l, p, kind], partner).wait_recv()

    def full3(l):
        send_full(rings3[l])
        for p in range(3):
            hand(l, p, 0)

    def forward3(l):
        for kind in (0, 1):
            for p, (copy, arrived) in enumerate(rings3[l]):
                arrived(kind)
                go(copy(kind + 2))
                hand(l, p, kind + 1)

    def finish3(l):
        for kind in (2, 3):
            for p, (_, arrived) in enumerate(rings3[l]):
                arrived(kind)
                hand(l, p, kind + 1)

    end_spread(spreads2[0])
    full3(0)
    handed(0, (0,))
    go(remote(core_rows, far, sh.at[1], rh.at[1], across))
    end_spread(spreads2[1])
    full3(1)
    forward3(0)
    full3(2)

    for k in range(3):
        origin = wrap(x - (k + 1), 4)
        part = T.at[origin, share]
        remote(part, part, sp_.at[0, k], rp_.at[0, k], x_peers[k]).wait_recv()
        go(remote(part, part, sp_.at[1, k], rp_.at[1, k], partner))

    def norm(l):
        low, rows = STEP * l, 192 - 2 * STEP * l
        src = X if l == 0 else Y
        g = gainv[l : l + 1, :]

        @pl.loop(0, rows // 16)
        def _(i):
            r = pl.multiple_of(low + i * 16, 16)
            v = src[pl.ds(r, 16), :].astype(F32)
            scaled = v * lax.rsqrt(jnp.mean(v * v, axis=-1, keepdims=True) + EPSILON)
            N[pl.ds(r, 16), :] = (scaled * g).astype(BF16)

    def project(l, p, dst):
        low, rows = STEP * l, 192 - 2 * STEP * l
        w = W[l, p].reshape(1024, 512)
        dst[pl.ds(low, rows), :] = jnp.dot(N[pl.ds(low, rows), :], w, preferred_element_type=F32)

    def gating(l):
        low, rows = STEP * l, 192 - 2 * STEP * l

        @pl.loop(0, rows // 16)
        def _(i):
            r = pl.multiple_of(low + i * 16, 16)
            at = pl.ds(r, 16)
            g = (V[at, :] * jax.nn.sigmoid(G[at, :])).astype(BF16).astype(F32)
            where = sp * 64 - 64 + r + lax.broadcasted_iota(jnp.int32, (16, 512), 0)
            g = jnp.where((where >= 0) & (where < 2048), g, 0.0)
            for j in range(4):
                GT[j, at, :] = g[:, 128 * j : 128 * j + 128]

    def conv(l):
        low, rows = STEP * (l + 1), 192 - 2 * STEP * (l + 1)
        for j in range(4):
            for r in range(low, low + rows, CHUNK):
                acc = jnp.zeros((CHUNK, 128), F32) + T[j, TAPS, l : l + 1, :]
                for k in range(TAPS):
                    acc = acc + GT[j, r + k - 15 : r + k - 15 + CHUNK, :] * T[j, k, l : l + 1, :]
                CV[r : r + CHUNK, 128 * j : 128 * j + 128] = acc

    def channel_norm(l):
        low, rows = STEP * (l + 1), 192 - 2 * STEP * (l + 1)
        g = jnp.concatenate([T[j, TAPS + 1, l : l + 1, :] for j in range(4)], axis=1)
        b = jnp.concatenate([T[j, TAPS + 2, l : l + 1, :] for j in range(4)], axis=1)

        @pl.loop(0, rows // 16)
        def _(i):
            at = pl.ds(pl.multiple_of(low + i * 16, 16), 16)
            v = CV[at, :]
            centered = v - jnp.mean(v, axis=-1, keepdims=True)
            spread = jnp.mean(centered * centered, axis=-1, keepdims=True)
            v = centered * lax.rsqrt(spread + EPSILON) * g + b
            A[at, :] = (v * jax.nn.sigmoid(v)).astype(BF16)

    def output(l):
        low, rows = STEP * (l + 1), 192 - 2 * STEP * (l + 1)
        src = X if l == 0 else Y
        for q in range(4):
            w = W[l, 2, q].reshape(256, 512)
            branch = lax.dot_general(
                A[pl.ds(low, rows), :], w, (((1,), (1,)), ((), ())), preferred_element_type=F32
            )
            lanes = slice(256 * q, 256 * q + 256)
            total = (src[low : low + rows, lanes].astype(F32) + branch).astype(BF16)
            if l + 1 < LAYERS:
                Y[low : low + rows, lanes] = total
            else:
                O[q] = total

    def compute(l, between=()):
        steps = [
            functools.partial(norm, l),
            functools.partial(project, l, 0, V),
            functools.partial(project, l, 1, G),
            functools.partial(gating, l),
            functools.partial(conv, l),
            functools.partial(channel_norm, l),
            functools.partial(output, l),
        ]
        between = dict(between)
        for i, step in enumerate(steps):
            if i in between:
                between[i]()
            step()

    forward3(1)
    finish3(0)
    full3(3)
    handed(0, (1, 2, 3, 4))
    for k in range(3):
        origin = wrap(x - (k + 1), 4)
        part = T.at[origin, pl.ds(17 - 17 * c, 17)]
        remote(part, part, sp_.at[1, k], rp_.at[1, k], partner).wait_recv()
    remote(core_rows, far, sh.at[0], rh.at[0], partner).wait_recv()
    remote(core_rows, near, sh.at[1], rh.at[1], across).wait_recv()
    compute(0, {3: lambda: forward3(2), 5: lambda: finish3(1)})
    handed(1)
    compute(1, {3: lambda: forward3(3), 5: lambda: finish3(2)})
    handed(2)
    compute(2, {5: lambda: finish3(3)})
    handed(3)
    compute(3)

    mine = pltpu.make_async_copy(O.at[x], out.at[x], loc.at[10])
    mine.start()
    for k, to in enumerate(x_peers):
        go(remote(O.at[to[1]], out.at[x], so.at[k], ro.at[k], to))
    for k in range(3):
        part = out.at[wrap(x - (k + 1), 4)]
        remote(O.at[0], part, so.at[k], ro.at[k], x_peers[k]).wait_recv()
    mine.wait()
    for copy in sends:
        copy.wait_send()


def shards(tokens, norm_gain, val_weight, gate_weight, conv_taps, conv_bias, ln_gain, ln_shift, out_weight):
    any_ = pl.BlockSpec(memory_space=pltpu.HBM)
    dma = pltpu.SemaphoreType.DMA
    vmem = pltpu.VMEM
    return pl.pallas_call(
        kernel,
        name="conv_stack",
        out_shape=jax.ShapeDtypeStruct(tokens.shape, tokens.dtype),
        in_specs=[any_] * 9,
        out_specs=pl.BlockSpec(memory_space=pl.ANY),
        scratch_shapes=[
            vmem((LAYERS, 3, 4, 4, 2, 32, 512), BF16),
            vmem((192, 1024), BF16),
            vmem((192, 1024), BF16),
            vmem((192, 1024), BF16),
            vmem((192, 512), F32),
            vmem((192, 512), F32),
            vmem((4, 192, 128), F32),
            vmem((192, 512), F32),
            vmem((192, 512), BF16),
            vmem((4, 64, 256), BF16),
            vmem((LAYERS, 1024), F32),
            vmem((4, TAPS + 3, LAYERS, 128), F32),
            dma((11,)),
            dma((2, 3, 3)), dma((2, 3, 3)),
            dma((2, 3, 3)), dma((2, 3, 3)),
            dma((LAYERS, 3, 4)), dma((LAYERS, 3, 4)),
            dma((LAYERS, 3, 5)), dma((LAYERS, 3, 5)),
            dma((3,)), dma((3,)),
            dma((2,)), dma((2,)),
            dma((2, 3)), dma((2, 3)),
            dma((3,)), dma((3,)),
        ],
        compiler_params=pltpu.CompilerParams(
            collective_id=0, has_side_effects=True, vmem_limit_bytes=67043328
        ),
    )(
        tokens, norm_gain, val_weight, gate_weight, conv_taps.transpose(1, 0, 2), conv_bias, ln_gain, ln_shift,
        out_weight.transpose(0, 2, 1),
    )


def solution(mesh):
    return jax.shard_map(
        shards,
        mesh=mesh,
        in_specs=(
            P(None, "sp", "tp"),
            P(),
            P(None, "sp", "tp"),
            P(None, "sp", "tp"),
            P(None, None, "tp"),
            P(None, "tp"),
            P(None, "tp"),
            P(None, "tp"),
            P(None, "tp", "sp"),
        ),
        out_specs=P(None, "sp", "tp"),
        check_vma=False,
    )
```

```python
import functools

import jax
import jax.numpy as jnp
from jax import lax
from jax.experimental import pallas as pl
from jax.experimental.pallas import tpu as pltpu
from jax.sharding import PartitionSpec as P

LAYERS = 4
EPSILON = 1e-06
STEP = 16
TAPS = 31
MESH = pl.DeviceIdType.MESH
F32, BF16 = jnp.float32, jnp.bfloat16
ORDERS = (("x", "y", "z"), ("y", "z", "x"), ("z", "x", "y"))
GROUPS1 = ((0, 1), (1, 3))
GROUPS2 = ((0, 1), (1, 1), (2, 2))
CHUNK = 32
NORM_CHUNK = 32


def wrap(v, n):
    return lax.rem(v + n, n)


def kernel(
    tok, gain, val, gate, taps, bias, lng, lnb, outw, out,
    W, X, Y, N, V, G, GT, CV, A, O, gainv, T,
    loc, s1, r1, s2, r2, s3, r3, sd, rd, st, rt, sh, rh, sp_, rp_, so, ro,
):
    sp = lax.axis_index("sp")
    x = lax.axis_index("tp")
    n_sp = 32
    c = lax.rem(sp, 2)
    y = lax.rem(sp // 2, 4)
    z = sp // 8
    me = {"x": x, "y": y, "z": z}

    def device(d, step):
        at = dict(me)
        at[d] = wrap(me[d] + step, 4)
        return ((at["z"] * 4 + at["y"]) * 2 + c, at["x"])

    partner = (sp + 1 - 2 * c, x)
    across = (wrap(sp + 1 - 2 * (1 - c), n_sp), x)
    x_peers = [(sp, wrap(x + k, 4)) for k in (1, 2, 3)]

    barrier = pltpu.get_barrier_semaphore()
    peers = [device(d, step) for d in "xyz" for step in (1, 2, 3)] + [partner]
    for peer in peers:
        pl.semaphore_signal(barrier, inc=1, device_id=peer, device_id_type=MESH)

    cols = lambda i, w: pl.ds(pl.multiple_of(i * w, w), w)
    parts = (val, gate, outw)
    starts = [pltpu.make_async_copy(w, W.at[:, p, z, y, c, :, cols(x, 128)], loc.at[p]) for p, w in enumerate(parts)]
    starts += [
        pltpu.make_async_copy(tok.at[x], X.at[pl.ds(64, 64), cols(x, 256)], loc.at[3]),
        pltpu.make_async_copy(gain, gainv, loc.at[4]),
        pltpu.make_async_copy(taps, T.at[x, pl.ds(0, TAPS)], loc.at[5]),
        pltpu.make_async_copy(bias, T.at[x, TAPS], loc.at[6]),
        pltpu.make_async_copy(lng, T.at[x, TAPS + 1], loc.at[7]),
        pltpu.make_async_copy(lnb, T.at[x, TAPS + 2], loc.at[8]),
    ]
    for copy in starts:
        copy.start()
    for copy in starts:
        copy.wait()
    pl.semaphore_wait(barrier, len(peers))

    sends = []

    def region(first, count, p, at, core, half):
        pick = lambda v: slice(None) if v is None else v
        rows = slice(None) if half is None else pl.ds(16 * half, 16)
        lanes = slice(None) if at["x"] is None else cols(at["x"], 128)
        return W.at[pl.ds(first, count), p, pick(at["z"]), pick(at["y"]), core, rows, lanes]

    def held(p, phase, coordinate):
        at = dict(me)
        for d in ORDERS[p][:phase]:
            at[d] = None
        at[ORDERS[p][phase]] = coordinate
        return at

    def remote(src, dst, ssem, rsem, to):
        return pltpu.make_async_remote_copy(
            src_ref=src, dst_ref=dst, send_sem=ssem, recv_sem=rsem, device_id=to, device_id_type=MESH
        )

    def ring(p, phase, first, count, ssem, rsem):
        d = ORDERS[p][phase]
        mine = me[d]
        kinds = ((1, 0, 1), (-1, 1, 1), (1, 1, 1), (-1, 0, 1), (1, 0, 2), (-1, 1, 2))

        def copy(kind):
            step, half, hops = kinds[kind]
            part = region(first, count, p, held(p, phase, wrap(mine - step * (hops - 1), 4)), c, half)
            return remote(part, part, ssem.at[kind], rsem.at[kind], device(d, step))

        def arrived(kind):
            step, half, hops = kinds[kind]
            part = region(first, count, p, held(p, phase, wrap(mine - step * hops, 4)), c, half)
            remote(part, part, ssem.at[kind], rsem.at[kind], device(d, step)).wait_recv()

        return copy, arrived

    def go(copy):
        copy.start()
        sends.append(copy)

    def spread(p, phase, first, count, ssem, rsem):
        d = ORDERS[p][phase]

        def copy(k):
            part = region(first, count, p, held(p, phase, me[d]), c, None)
            return remote(part, part, ssem.at[k - 1], rsem.at[k - 1], device(d, k))

        def arrived(k):
            part = region(first, count, p, held(p, phase, wrap(me[d] - k, 4)), c, None)
            remote(part, part, ssem.at[k - 1], rsem.at[k - 1], device(d, k)).wait_recv()

        return copy, arrived

    spreads1 = [[spread(p, 0, f, n, s1.at[g, p], r1.at[g, p]) for p in range(3)] for g, (f, n) in enumerate(GROUPS1)]
    spreads2 = [[spread(p, 1, f, n, s2.at[g, p], r2.at[g, p]) for p in range(3)] for g, (f, n) in enumerate(GROUPS2)]
    rings3 = [[ring(p, 2, l, 1, s3.at[l, p], r3.at[l, p]) for p in range(3)] for l in range(LAYERS)]

    def send_spread(spreads):
        for k in (2, 1, 3):
            for copy, _ in spreads:
                go(copy(k))

    def end_spread(spreads):
        for k in (1, 3, 2):
            for _, arrived in spreads:
                arrived(k)

    def send_tokens(k):
        go(remote(tok.at[x_peers[k][1]], X.at[pl.ds(64, 64), cols(x, 256)], st.at[k], rt.at[k], x_peers[k]))

    share = pl.ds(17 * c, 17)

    def send_parameters(k):
        go(remote(T.at[x, share], T.at[x, share], sp_.at[0, k], rp_.at[0, k], x_peers[k]))

    send_spread(spreads1[0])
    send_spread(spreads1[1])
    for k in (1, 0, 2):
        send_tokens(k)
    for k in (1, 0, 2):
        send_parameters(k)
    end_spread(spreads1[0])
    send_spread(spreads2[0])
    end_spread(spreads1[1])
    send_spread(spreads2[1])
    send_spread(spreads2[2])
    for k in range(3):
        part = X.at[pl.ds(64, 64), cols(wrap(x - (k + 1), 4), 256)]
        remote(part, part, st.at[k], rt.at[k], x_peers[k]).wait_recv()
    core_rows = X.at[pl.ds(64, 64)]
    near = X.at[pl.ds(128 * c, 64)]
    far = X.at[pl.ds(128 - 128 * c, 64)]
    go(remote(core_rows, near, sh.at[0], rh.at[0], partner))

    def hand(l, p, kind):
        step, half = ((0, None), (1, None), (-1, None), (2, 0), (2, 1))[kind]
        at = held(p, 2, wrap(me[ORDERS[p][2]] - step, 4))
        part = region(l, 1, p, at, c, half)
        go(remote(part, part, sd.at[l, p, kind], rd.at[l, p, kind], partner))

    def handed(l, kinds=(0, 1, 2, 3, 4)):
        for kind in kinds:
            step, half = ((0, None), (1, None), (-1, None), (2, 0), (2, 1))[kind]
            for p in range(3):
                at = held(p, 2, wrap(me[ORDERS[p][2]] - step, 4))
                part = region(l, 1, p, at, 1 - c, half)
                remote(part, part, sd.at[l, p, kind], rd.at[l, p, kind], partner).wait_recv()

    def first3(l):
        for kind in (0, 1):
            for copy, _ in rings3[l]:
                go(copy(kind))

    def second3(l):
        for kind in (2, 3):
            for copy, _ in rings3[l]:
                go(copy(kind))
        for p in range(3):
            hand(l, p, 0)

    def forward3(l):
        for kind in (0, 1):
            for copy, arrived in rings3[l]:
                arrived(kind)
                go(copy(kind + 4))

    def planes3(l):
        for kind in (2, 3):
            for p, (_, arrived) in enumerate(rings3[l]):
                arrived(kind)
                hand(l, p, kind - 1)

    def finish3(l):
        for kind in (4, 5):
            for p, (_, arrived) in enumerate(rings3[l]):
                arrived(kind)
                hand(l, p, kind - 1)

    def parameters():
        for k in range(3):
            part = T.at[wrap(x - (k + 1), 4), share]
            remote(part, part, sp_.at[0, k], rp_.at[0, k], x_peers[k]).wait_recv()
            go(remote(part, part, sp_.at[1, k], rp_.at[1, k], partner))

    def parameters_here():
        for k in range(3):
            part = T.at[wrap(x - (k + 1), 4), pl.ds(17 - 17 * c, 17)]
            remote(part, part, sp_.at[1, k], rp_.at[1, k], partner).wait_recv()

    def halo_across():
        handed(0, (0,))
        go(remote(core_rows, far, sh.at[1], rh.at[1], across))

    def halo_here():
        remote(core_rows, far, sh.at[0], rh.at[0], partner).wait_recv()
        remote(core_rows, near, sh.at[1], rh.at[1], across).wait_recv()

    def norm(l):
        low, rows = STEP * l, 192 - 2 * STEP * l
        src = X if l == 0 else Y
        g = gainv[l : l + 1, :]

        for r in range(low, low + rows, NORM_CHUNK):
            at = pl.ds(r, NORM_CHUNK)
            v = src[at, :].astype(F32)
            scaled = v * lax.rsqrt(jnp.mean(v * v, axis=-1, keepdims=True) + EPSILON)
            N[at, :] = (scaled * g).astype(BF16)

    def project(l, p, dst):
        low, rows = STEP * l, 192 - 2 * STEP * l
        w = W[l, p].reshape(1024, 512)
        dst[pl.ds(low, rows), :] = jnp.dot(N[pl.ds(low, rows), :], w, preferred_element_type=F32)

    def gating(l):
        low, rows = STEP * l, 192 - 2 * STEP * l

        for r in range(low, low + rows, CHUNK):
            at = pl.ds(r, CHUNK)
            g = (V[at, :] * jax.nn.sigmoid(G[at, :])).astype(BF16).astype(F32)
            if r < 64 or r + CHUNK > 128:
                where = sp * 64 - 64 + r + lax.broadcasted_iota(jnp.int32, (CHUNK, 512), 0)
                g = jnp.where((where >= 0) & (where < 2048), g, 0.0)
            for j in range(4):
                GT[j, at, :] = g[:, 128 * j : 128 * j + 128]

    def conv(l):
        low, rows = STEP * (l + 1), 192 - 2 * STEP * (l + 1)
        for j in range(4):
            for r in range(low, low + rows, CHUNK):
                acc = jnp.zeros((CHUNK, 128), F32) + T[j, TAPS, l : l + 1, :]
                for k in range(TAPS):
                    acc = acc + GT[j, r + k - 15 : r + k - 15 + CHUNK, :] * T[j, k, l : l + 1, :]
                CV[r : r + CHUNK, 128 * j : 128 * j + 128] = acc

    def channel_norm(l):
        low, rows = STEP * (l + 1), 192 - 2 * STEP * (l + 1)
        g = jnp.concatenate([T[j, TAPS + 1, l : l + 1, :] for j in range(4)], axis=1)
        b = jnp.concatenate([T[j, TAPS + 2, l : l + 1, :] for j in range(4)], axis=1)

        for r in range(low, low + rows, CHUNK):
            at = pl.ds(r, CHUNK)
            v = CV[at, :]
            centered = v - jnp.mean(v, axis=-1, keepdims=True)
            spread = jnp.mean(centered * centered, axis=-1, keepdims=True)
            v = centered * lax.rsqrt(spread + EPSILON) * g + b
            A[at, :] = (v * jax.nn.sigmoid(v)).astype(BF16)

    def output(l):
        low, rows = STEP * (l + 1), 192 - 2 * STEP * (l + 1)
        src = X if l == 0 else Y
        for q in range(4):
            w = W[l, 2, q].reshape(256, 512)
            branch = lax.dot_general(
                A[pl.ds(low, rows), :], w, (((1,), (1,)), ((), ())), preferred_element_type=F32
            )
            lanes = slice(256 * q, 256 * q + 256)
            total = (src[low : low + rows, lanes].astype(F32) + branch).astype(BF16)
            if l + 1 < LAYERS:
                Y[low : low + rows, lanes] = total
            else:
                O[q] = total

    def compute(l, first=0, last=7):
        steps = (
            norm,
            lambda l: project(l, 0, V),
            lambda l: project(l, 1, G),
            gating,
            conv,
            channel_norm,
            output,
        )
        for step in steps[first:last]:
            step(l)

    end_spread(spreads2[0])
    first3(0)
    second3(0)
    halo_across()
    end_spread(spreads2[1])
    first3(1)
    second3(1)
    parameters()
    end_spread(spreads2[2])
    forward3(0)
    first3(2)
    first3(3)
    planes3(0)
    forward3(1)
    second3(2)
    planes3(1)
    finish3(0)
    halo_here()
    norm(0)
    forward3(2)
    second3(3)
    parameters_here()
    handed(0, (1, 2, 3, 4))
    compute(0, 1, 4)
    forward3(3)
    compute(0, 4, 7)
    finish3(1)
    planes3(2)
    handed(1)
    compute(1, 0, 3)
    finish3(2)
    compute(1, 3, 7)
    planes3(3)
    handed(2)
    compute(2, 0, 3)
    finish3(3)
    compute(2, 3, 7)
    norm(3)
    handed(3)
    compute(3, 1, 7)

    mine = pltpu.make_async_copy(O.at[x], out.at[x], loc.at[10])
    mine.start()
    for k, to in enumerate(x_peers):
        go(remote(O.at[to[1]], out.at[x], so.at[k], ro.at[k], to))
    for k in range(3):
        part = out.at[wrap(x - (k + 1), 4)]
        remote(O.at[0], part, so.at[k], ro.at[k], x_peers[k]).wait_recv()
    mine.wait()
    for copy in sends:
        copy.wait_send()


def shards(tokens, norm_gain, val_weight, gate_weight, conv_taps, conv_bias, ln_gain, ln_shift, out_weight):
    any_ = pl.BlockSpec(memory_space=pltpu.HBM)
    dma = pltpu.SemaphoreType.DMA
    vmem = pltpu.VMEM
    return pl.pallas_call(
        kernel,
        name="conv_stack",
        out_shape=jax.ShapeDtypeStruct(tokens.shape, tokens.dtype),
        in_specs=[any_] * 9,
        out_specs=pl.BlockSpec(memory_space=pl.ANY),
        scratch_shapes=[
            vmem((LAYERS, 3, 4, 4, 2, 32, 512), BF16),
            vmem((192, 1024), BF16),
            vmem((192, 1024), BF16),
            vmem((192, 1024), BF16),
            vmem((192, 512), F32),
            vmem((192, 512), F32),
            vmem((4, 192, 128), F32),
            vmem((192, 512), F32),
            vmem((192, 512), BF16),
            vmem((4, 64, 256), BF16),
            vmem((LAYERS, 1024), F32),
            vmem((4, TAPS + 3, LAYERS, 128), F32),
            dma((11,)),
            dma((2, 3, 3)), dma((2, 3, 3)),
            dma((3, 3, 3)), dma((3, 3, 3)),
            dma((LAYERS, 3, 6)), dma((LAYERS, 3, 6)),
            dma((LAYERS, 3, 5)), dma((LAYERS, 3, 5)),
            dma((3,)), dma((3,)),
            dma((2,)), dma((2,)),
            dma((2, 3)), dma((2, 3)),
            dma((3,)), dma((3,)),
        ],
        compiler_params=pltpu.CompilerParams(
            collective_id=0, has_side_effects=True, vmem_limit_bytes=67043328
        ),
    )(
        tokens, norm_gain, val_weight, gate_weight, conv_taps.transpose(1, 0, 2), conv_bias, ln_gain, ln_shift,
        out_weight.transpose(0, 2, 1),
    )


def solution(mesh):
    return jax.shard_map(
        shards,
        mesh=mesh,
        in_specs=(
            P(None, "sp", "tp"),
            P(),
            P(None, "sp", "tp"),
            P(None, "sp", "tp"),
            P(None, None, "tp"),
            P(None, "tp"),
            P(None, "tp"),
            P(None, "tp"),
            P(None, "tp", "sp"),
        ),
        out_specs=P(None, "sp", "tp"),
        check_vma=False,
    )
```

```python
import functools

import jax
import jax.numpy as jnp
from jax import lax
from jax.experimental import pallas as pl
from jax.experimental.pallas import tpu as pltpu
from jax.sharding import PartitionSpec as P

LAYERS = 4
EPSILON = 1e-06
STEP = 16
TAPS = 31
MESH = pl.DeviceIdType.MESH
F32, BF16 = jnp.float32, jnp.bfloat16
ORDERS = (("x", "y", "z"), ("y", "z", "x"), ("z", "x", "y"))
GROUPS1 = ((0, 1), (1, 3))
GROUPS2 = ((0, 1), (1, 1), (2, 2))
CHUNK = 32
NORM_CHUNK = 32


def wrap(v, n):
    return lax.rem(v + n, n)


def kernel(
    tok, gain, val, gate, taps, bias, lng, lnb, outw, out,
    W, X, Y, N, V, G, GT, CV, A, O, gainv, T,
    loc, s1, r1, s2, r2, s3, r3, sd, rd, st, rt, sh, rh, sp_, rp_, so, ro,
):
    sp = lax.axis_index("sp")
    x = lax.axis_index("tp")
    n_sp = 32
    c = lax.rem(sp, 2)
    y = lax.rem(sp // 2, 4)
    z = sp // 8
    me = {"x": x, "y": y, "z": z}

    def device(d, step):
        at = dict(me)
        at[d] = wrap(me[d] + step, 4)
        return ((at["z"] * 4 + at["y"]) * 2 + c, at["x"])

    partner = (sp + 1 - 2 * c, x)
    across = (wrap(sp + 1 - 2 * (1 - c), n_sp), x)
    x_peers = [(sp, wrap(x + k, 4)) for k in (1, 2, 3)]

    barrier = pltpu.get_barrier_semaphore()
    peers = [device(d, step) for d in "xyz" for step in (1, 2, 3)] + [partner]
    for peer in peers:
        pl.semaphore_signal(barrier, inc=1, device_id=peer, device_id_type=MESH)

    cols = lambda i, w: pl.ds(pl.multiple_of(i * w, w), w)
    parts = (val, gate, outw)
    starts = [pltpu.make_async_copy(w, W.at[:, p, z, y, c, :, cols(x, 128)], loc.at[p]) for p, w in enumerate(parts)]
    starts += [
        pltpu.make_async_copy(tok.at[x], X.at[pl.ds(64, 64), cols(x, 256)], loc.at[3]),
        pltpu.make_async_copy(gain, gainv, loc.at[4]),
        pltpu.make_async_copy(taps, T.at[x, pl.ds(0, TAPS)], loc.at[5]),
        pltpu.make_async_copy(bias, T.at[x, TAPS], loc.at[6]),
        pltpu.make_async_copy(lng, T.at[x, TAPS + 1], loc.at[7]),
        pltpu.make_async_copy(lnb, T.at[x, TAPS + 2], loc.at[8]),
    ]
    for copy in starts:
        copy.start()
    for copy in starts:
        copy.wait()
    pl.semaphore_wait(barrier, len(peers))

    sends = []

    def region(first, count, p, at, core, half):
        pick = lambda v: slice(None) if v is None else v
        rows = slice(None) if half is None else pl.ds(16 * half, 16)
        lanes = slice(None) if at["x"] is None else cols(at["x"], 128)
        return W.at[pl.ds(first, count), p, pick(at["z"]), pick(at["y"]), core, rows, lanes]

    def held(p, phase, coordinate):
        at = dict(me)
        for d in ORDERS[p][:phase]:
            at[d] = None
        at[ORDERS[p][phase]] = coordinate
        return at

    def remote(src, dst, ssem, rsem, to):
        return pltpu.make_async_remote_copy(
            src_ref=src, dst_ref=dst, send_sem=ssem, recv_sem=rsem, device_id=to, device_id_type=MESH
        )

    def ring(p, phase, first, count, ssem, rsem):
        d = ORDERS[p][phase]
        mine = me[d]
        kinds = ((1, 0, 1), (-1, 1, 1), (1, 1, 1), (-1, 0, 1), (1, 0, 2), (-1, 1, 2))

        def copy(kind):
            step, half, hops = kinds[kind]
            part = region(first, count, p, held(p, phase, wrap(mine - step * (hops - 1), 4)), c, half)
            return remote(part, part, ssem.at[kind], rsem.at[kind], device(d, step))

        def arrived(kind):
            step, half, hops = kinds[kind]
            part = region(first, count, p, held(p, phase, wrap(mine - step * hops, 4)), c, half)
            remote(part, part, ssem.at[kind], rsem.at[kind], device(d, step)).wait_recv()

        return copy, arrived

    def go(copy):
        copy.start()
        sends.append(copy)

    def spread(p, phase, first, count, ssem, rsem):
        d = ORDERS[p][phase]

        def copy(k):
            part = region(first, count, p, held(p, phase, me[d]), c, None)
            return remote(part, part, ssem.at[k - 1], rsem.at[k - 1], device(d, k))

        def arrived(k):
            part = region(first, count, p, held(p, phase, wrap(me[d] - k, 4)), c, None)
            remote(part, part, ssem.at[k - 1], rsem.at[k - 1], device(d, k)).wait_recv()

        return copy, arrived

    spreads1 = [[spread(p, 0, f, n, s1.at[g, p], r1.at[g, p]) for p in range(3)] for g, (f, n) in enumerate(GROUPS1)]
    spreads2 = [[spread(p, 1, f, n, s2.at[g, p], r2.at[g, p]) for p in range(3)] for g, (f, n) in enumerate(GROUPS2)]
    rings3 = [[ring(p, 2, l, 1, s3.at[l, p], r3.at[l, p]) for p in range(3)] for l in range(LAYERS)]

    def send_spread(spreads):
        for k in (2, 1, 3):
            for copy, _ in spreads:
                go(copy(k))

    def end_spread(spreads):
        for k in (1, 3, 2):
            for _, arrived in spreads:
                arrived(k)

    def send_tokens(k):
        go(remote(tok.at[x_peers[k][1]], X.at[pl.ds(64, 64), cols(x, 256)], st.at[k], rt.at[k], x_peers[k]))

    share = pl.ds(17 * c, 17)

    def send_parameters(k):
        go(remote(T.at[x, share], T.at[x, share], sp_.at[0, k], rp_.at[0, k], x_peers[k]))

    send_spread(spreads1[0])
    send_spread(spreads1[1])
    for k in (1, 0, 2):
        send_tokens(k)
    for k in (1, 0, 2):
        send_parameters(k)
    end_spread(spreads1[0])
    send_spread(spreads2[0])
    end_spread(spreads1[1])
    send_spread(spreads2[1])
    send_spread(spreads2[2])
    for k in range(3):
        part = X.at[pl.ds(64, 64), cols(wrap(x - (k + 1), 4), 256)]
        remote(part, part, st.at[k], rt.at[k], x_peers[k]).wait_recv()
    core_rows = X.at[pl.ds(64, 64)]
    near = X.at[pl.ds(128 * c, 64)]
    far = X.at[pl.ds(128 - 128 * c, 64)]
    go(remote(core_rows, near, sh.at[0], rh.at[0], partner))

    def hand(l, p, kind):
        step, half = ((0, None), (1, None), (-1, None), (2, 0), (2, 1))[kind]
        at = held(p, 2, wrap(me[ORDERS[p][2]] - step, 4))
        part = region(l, 1, p, at, c, half)
        go(remote(part, part, sd.at[l, p, kind], rd.at[l, p, kind], partner))

    def handed(l, kinds=(0, 1, 2, 3, 4), parts=(0, 1, 2)):
        for kind in kinds:
            step, half = ((0, None), (1, None), (-1, None), (2, 0), (2, 1))[kind]
            for p in parts:
                at = held(p, 2, wrap(me[ORDERS[p][2]] - step, 4))
                part = region(l, 1, p, at, 1 - c, half)
                remote(part, part, sd.at[l, p, kind], rd.at[l, p, kind], partner).wait_recv()

    def first3(l):
        for kind in (0, 1):
            for copy, _ in rings3[l]:
                go(copy(kind))

    def second3(l):
        for kind in (2, 3):
            for copy, _ in rings3[l]:
                go(copy(kind))
        for p in range(3):
            hand(l, p, 0)

    def forward3(l):
        for kind in (0, 1):
            for copy, arrived in rings3[l]:
                arrived(kind)
                go(copy(kind + 4))

    def planes3(l):
        for kind in (2, 3):
            for p, (_, arrived) in enumerate(rings3[l]):
                arrived(kind)
                hand(l, p, kind - 1)

    def finish3(l):
        for kind in (4, 5):
            for p, (_, arrived) in enumerate(rings3[l]):
                arrived(kind)
                hand(l, p, kind - 1)

    def parameters():
        for k in range(3):
            part = T.at[wrap(x - (k + 1), 4), share]
            remote(part, part, sp_.at[0, k], rp_.at[0, k], x_peers[k]).wait_recv()
            go(remote(part, part, sp_.at[1, k], rp_.at[1, k], partner))

    def parameters_here():
        for k in range(3):
            part = T.at[wrap(x - (k + 1), 4), pl.ds(17 - 17 * c, 17)]
            remote(part, part, sp_.at[1, k], rp_.at[1, k], partner).wait_recv()

    def halo_across():
        handed(0, (0,))
        go(remote(core_rows, far, sh.at[1], rh.at[1], across))

    def halo_here():
        remote(core_rows, far, sh.at[0], rh.at[0], partner).wait_recv()
        remote(core_rows, near, sh.at[1], rh.at[1], across).wait_recv()

    def norm(l):
        low, rows = STEP * l, 192 - 2 * STEP * l
        src = X if l == 0 else Y
        g = gainv[l : l + 1, :]

        for r in range(low, low + rows, NORM_CHUNK):
            at = pl.ds(r, NORM_CHUNK)
            v = src[at, :].astype(F32)
            scaled = v * lax.rsqrt(jnp.mean(v * v, axis=-1, keepdims=True) + EPSILON)
            N[at, :] = (scaled * g).astype(BF16)

    def project(l, p, dst):
        low, rows = STEP * l, 192 - 2 * STEP * l
        w = W[l, p].reshape(1024, 512)
        dst[pl.ds(low, rows), :] = jnp.dot(N[pl.ds(low, rows), :], w, preferred_element_type=F32)

    def gating(l):
        low, rows = STEP * l, 192 - 2 * STEP * l

        for r in range(low, low + rows, CHUNK):
            at = pl.ds(r, CHUNK)
            g = (V[at, :] * jax.nn.sigmoid(G[at, :])).astype(BF16).astype(F32)
            if r < 64 or r + CHUNK > 128:
                where = sp * 64 - 64 + r + lax.broadcasted_iota(jnp.int32, (CHUNK, 512), 0)
                g = jnp.where((where >= 0) & (where < 2048), g, 0.0)
            for j in range(4):
                GT[j, at, :] = g[:, 128 * j : 128 * j + 128]

    def conv(l):
        low, rows = STEP * (l + 1), 192 - 2 * STEP * (l + 1)
        for j in range(4):
            for r in range(low, low + rows, CHUNK):
                acc = jnp.zeros((CHUNK, 128), F32) + T[j, TAPS, l : l + 1, :]
                for k in range(TAPS):
                    acc = acc + GT[j, r + k - 15 : r + k - 15 + CHUNK, :] * T[j, k, l : l + 1, :]
                CV[r : r + CHUNK, 128 * j : 128 * j + 128] = acc

    def channel_norm(l):
        low, rows = STEP * (l + 1), 192 - 2 * STEP * (l + 1)
        g = jnp.concatenate([T[j, TAPS + 1, l : l + 1, :] for j in range(4)], axis=1)
        b = jnp.concatenate([T[j, TAPS + 2, l : l + 1, :] for j in range(4)], axis=1)

        for r in range(low, low + rows, CHUNK):
            at = pl.ds(r, CHUNK)
            v = CV[at, :]
            centered = v - jnp.mean(v, axis=-1, keepdims=True)
            spread = jnp.mean(centered * centered, axis=-1, keepdims=True)
            v = centered * lax.rsqrt(spread + EPSILON) * g + b
            A[at, :] = (v * jax.nn.sigmoid(v)).astype(BF16)

    def output(l):
        low, rows = STEP * (l + 1), 192 - 2 * STEP * (l + 1)
        src = X if l == 0 else Y
        for q in range(4):
            w = W[l, 2, q].reshape(256, 512)
            branch = lax.dot_general(
                A[pl.ds(low, rows), :], w, (((1,), (1,)), ((), ())), preferred_element_type=F32
            )
            lanes = slice(256 * q, 256 * q + 256)
            total = (src[low : low + rows, lanes].astype(F32) + branch).astype(BF16)
            if l + 1 < LAYERS:
                Y[low : low + rows, lanes] = total
            else:
                O[q] = total

    def compute(l, first=0, last=7):
        steps = (
            norm,
            lambda l: project(l, 0, V),
            lambda l: project(l, 1, G),
            gating,
            conv,
            channel_norm,
            output,
        )
        for step in steps[first:last]:
            step(l)

    end_spread(spreads2[0])
    first3(0)
    second3(0)
    halo_across()
    end_spread(spreads2[1])
    first3(1)
    second3(1)
    parameters()
    end_spread(spreads2[2])
    forward3(0)
    first3(2)
    first3(3)
    planes3(0)
    forward3(1)
    second3(2)
    planes3(1)
    finish3(0)
    halo_here()
    norm(0)
    forward3(2)
    second3(3)
    parameters_here()
    handed(0, (1, 2, 3, 4), (0, 1))
    compute(0, 1, 4)
    forward3(3)
    compute(0, 4, 6)
    handed(0, (1, 2, 3, 4), (2,))
    compute(0, 6, 7)
    finish3(1)
    planes3(2)
    norm(1)
    handed(1, parts=(0, 1))
    compute(1, 1, 3)
    finish3(2)
    compute(1, 3, 6)
    handed(1, parts=(2,))
    compute(1, 6, 7)
    planes3(3)
    norm(2)
    handed(2, parts=(0, 1))
    compute(2, 1, 3)
    finish3(3)
    compute(2, 3, 6)
    handed(2, parts=(2,))
    compute(2, 6, 7)
    norm(3)
    handed(3, parts=(0,))
    compute(3, 1, 2)
    handed(3, parts=(1,))
    compute(3, 2, 6)
    handed(3, parts=(2,))
    compute(3, 6, 7)

    mine = pltpu.make_async_copy(O.at[x], out.at[x], loc.at[10])
    mine.start()
    for k, to in enumerate(x_peers):
        go(remote(O.at[to[1]], out.at[x], so.at[k], ro.at[k], to))
    for k in range(3):
        part = out.at[wrap(x - (k + 1), 4)]
        remote(O.at[0], part, so.at[k], ro.at[k], x_peers[k]).wait_recv()
    mine.wait()
    for copy in sends:
        copy.wait_send()


def shards(tokens, norm_gain, val_weight, gate_weight, conv_taps, conv_bias, ln_gain, ln_shift, out_weight):
    any_ = pl.BlockSpec(memory_space=pltpu.HBM)
    dma = pltpu.SemaphoreType.DMA
    vmem = pltpu.VMEM
    return pl.pallas_call(
        kernel,
        name="conv_stack",
        out_shape=jax.ShapeDtypeStruct(tokens.shape, tokens.dtype),
        in_specs=[any_] * 9,
        out_specs=pl.BlockSpec(memory_space=pl.ANY),
        scratch_shapes=[
            vmem((LAYERS, 3, 4, 4, 2, 32, 512), BF16),
            vmem((192, 1024), BF16),
            vmem((192, 1024), BF16),
            vmem((192, 1024), BF16),
            vmem((192, 512), F32),
            vmem((192, 512), F32),
            vmem((4, 192, 128), F32),
            vmem((192, 512), F32),
            vmem((192, 512), BF16),
            vmem((4, 64, 256), BF16),
            vmem((LAYERS, 1024), F32),
            vmem((4, TAPS + 3, LAYERS, 128), F32),
            dma((11,)),
            dma((2, 3, 3)), dma((2, 3, 3)),
            dma((3, 3, 3)), dma((3, 3, 3)),
            dma((LAYERS, 3, 6)), dma((LAYERS, 3, 6)),
            dma((LAYERS, 3, 5)), dma((LAYERS, 3, 5)),
            dma((3,)), dma((3,)),
            dma((2,)), dma((2,)),
            dma((2, 3)), dma((2, 3)),
            dma((3,)), dma((3,)),
        ],
        compiler_params=pltpu.CompilerParams(
            collective_id=0, has_side_effects=True, vmem_limit_bytes=67043328
        ),
    )(
        tokens, norm_gain, val_weight, gate_weight, conv_taps.transpose(1, 0, 2), conv_bias, ln_gain, ln_shift,
        out_weight.transpose(0, 2, 1),
    )


def solution(mesh):
    return jax.shard_map(
        shards,
        mesh=mesh,
        in_specs=(
            P(None, "sp", "tp"),
            P(),
            P(None, "sp", "tp"),
            P(None, "sp", "tp"),
            P(None, None, "tp"),
            P(None, "tp"),
            P(None, "tp"),
            P(None, "tp"),
            P(None, "tp", "sp"),
        ),
        out_specs=P(None, "sp", "tp"),
        check_vma=False,
    )
```

```python
import functools

import jax
import jax.numpy as jnp
from jax import lax
from jax.experimental import pallas as pl
from jax.experimental.pallas import tpu as pltpu
from jax.sharding import PartitionSpec as P

LAYERS = 4
EPSILON = 1e-06
STEP = 16
TAPS = 31
MESH = pl.DeviceIdType.MESH
F32, BF16 = jnp.float32, jnp.bfloat16
ORDERS = (("x", "y", "z"), ("y", "z", "x"), ("z", "x", "y"))
GROUPS1 = ((0, 1), (1, 3))
GROUPS2 = ((0, 1), (1, 1), (2, 2))
CHUNK = 32
NORM_CHUNK = 32


def wrap(v, n):
    return lax.rem(v + n, n)


def kernel(
    tok, gain, val, gate, taps, bias, lng, lnb, outw, out,
    W, X, Y, N, V, G, GT, CV, A, O, gainv, T,
    loc, s1, r1, s2, r2, s3, r3, sd, rd, st, rt, sh, rh, sp_, rp_, so, ro,
):
    sp = lax.axis_index("sp")
    x = lax.axis_index("tp")
    n_sp = 32
    c = lax.rem(sp, 2)
    y = lax.rem(sp // 2, 4)
    z = sp // 8
    me = {"x": x, "y": y, "z": z}

    def device(d, step):
        at = dict(me)
        at[d] = wrap(me[d] + step, 4)
        return ((at["z"] * 4 + at["y"]) * 2 + c, at["x"])

    partner = (sp + 1 - 2 * c, x)
    across = (wrap(sp + 1 - 2 * (1 - c), n_sp), x)
    x_peers = [(sp, wrap(x + k, 4)) for k in (1, 2, 3)]

    barrier = pltpu.get_barrier_semaphore()
    peers = [device(d, step) for d in "xyz" for step in (1, 2, 3)] + [partner]
    for peer in peers:
        pl.semaphore_signal(barrier, inc=1, device_id=peer, device_id_type=MESH)

    cols = lambda i, w: pl.ds(pl.multiple_of(i * w, w), w)
    parts = (val, gate, outw)
    starts = [pltpu.make_async_copy(w, W.at[:, p, z, y, c, :, cols(x, 128)], loc.at[p]) for p, w in enumerate(parts)]
    starts += [
        pltpu.make_async_copy(tok.at[x], X.at[pl.ds(64, 64), cols(x, 256)], loc.at[3]),
        pltpu.make_async_copy(gain, gainv, loc.at[4]),
        pltpu.make_async_copy(taps, T.at[x, pl.ds(0, TAPS)], loc.at[5]),
        pltpu.make_async_copy(bias, T.at[x, TAPS], loc.at[6]),
        pltpu.make_async_copy(lng, T.at[x, TAPS + 1], loc.at[7]),
        pltpu.make_async_copy(lnb, T.at[x, TAPS + 2], loc.at[8]),
    ]
    for copy in starts:
        copy.start()
    for copy in starts:
        copy.wait()
    pl.semaphore_wait(barrier, len(peers))

    sends = []

    def region(first, count, p, at, core, half):
        pick = lambda v: slice(None) if v is None else v
        rows = slice(None) if half is None else pl.ds(16 * half, 16)
        lanes = slice(None) if at["x"] is None else cols(at["x"], 128)
        return W.at[pl.ds(first, count), p, pick(at["z"]), pick(at["y"]), core, rows, lanes]

    def held(p, phase, coordinate):
        at = dict(me)
        for d in ORDERS[p][:phase]:
            at[d] = None
        at[ORDERS[p][phase]] = coordinate
        return at

    def remote(src, dst, ssem, rsem, to):
        return pltpu.make_async_remote_copy(
            src_ref=src, dst_ref=dst, send_sem=ssem, recv_sem=rsem, device_id=to, device_id_type=MESH
        )

    def ring(p, phase, first, count, ssem, rsem):
        d = ORDERS[p][phase]
        mine = me[d]
        kinds = ((1, 0, 1), (-1, 1, 1), (1, 1, 1), (-1, 0, 1), (1, 0, 2), (-1, 1, 2))

        def copy(kind):
            step, half, hops = kinds[kind]
            part = region(first, count, p, held(p, phase, wrap(mine - step * (hops - 1), 4)), c, half)
            return remote(part, part, ssem.at[kind], rsem.at[kind], device(d, step))

        def arrived(kind):
            step, half, hops = kinds[kind]
            part = region(first, count, p, held(p, phase, wrap(mine - step * hops, 4)), c, half)
            remote(part, part, ssem.at[kind], rsem.at[kind], device(d, step)).wait_recv()

        return copy, arrived

    def go(copy):
        copy.start()
        sends.append(copy)

    def spread(p, phase, first, count, ssem, rsem):
        d = ORDERS[p][phase]

        def copy(k):
            part = region(first, count, p, held(p, phase, me[d]), c, None)
            return remote(part, part, ssem.at[k - 1], rsem.at[k - 1], device(d, k))

        def arrived(k):
            part = region(first, count, p, held(p, phase, wrap(me[d] - k, 4)), c, None)
            remote(part, part, ssem.at[k - 1], rsem.at[k - 1], device(d, k)).wait_recv()

        return copy, arrived

    spreads1 = [[spread(p, 0, f, n, s1.at[g, p], r1.at[g, p]) for p in range(3)] for g, (f, n) in enumerate(GROUPS1)]
    spreads2 = [[spread(p, 1, f, n, s2.at[g, p], r2.at[g, p]) for p in range(3)] for g, (f, n) in enumerate(GROUPS2)]
    rings3 = [[ring(p, 2, l, 1, s3.at[l, p], r3.at[l, p]) for p in range(3)] for l in range(LAYERS)]

    def send_spread(spreads):
        for k in (2, 1, 3):
            for copy, _ in spreads:
                go(copy(k))

    def end_spread(spreads):
        for k in (1, 3, 2):
            for _, arrived in spreads:
                arrived(k)

    def send_tokens(k):
        go(remote(tok.at[x_peers[k][1]], X.at[pl.ds(64, 64), cols(x, 256)], st.at[k], rt.at[k], x_peers[k]))

    share = pl.ds(17 * c, 17)

    def send_parameters(k):
        go(remote(T.at[x, share], T.at[x, share], sp_.at[0, k], rp_.at[0, k], x_peers[k]))

    send_spread(spreads1[0])
    send_spread(spreads1[1])
    for k in (1, 0, 2):
        send_tokens(k)
    for k in (1, 0, 2):
        send_parameters(k)
    end_spread(spreads1[0])
    send_spread(spreads2[0])
    end_spread(spreads1[1])
    send_spread(spreads2[1])
    send_spread(spreads2[2])
    for k in range(3):
        part = X.at[pl.ds(64, 64), cols(wrap(x - (k + 1), 4), 256)]
        remote(part, part, st.at[k], rt.at[k], x_peers[k]).wait_recv()
    core_rows = X.at[pl.ds(64, 64)]
    near = X.at[pl.ds(128 * c, 64)]
    far = X.at[pl.ds(128 - 128 * c, 64)]
    go(remote(core_rows, near, sh.at[0], rh.at[0], partner))

    def hand(l, p, kind):
        step, half = ((0, None), (1, None), (-1, None), (2, 0), (2, 1))[kind]
        at = held(p, 2, wrap(me[ORDERS[p][2]] - step, 4))
        part = region(l, 1, p, at, c, half)
        go(remote(part, part, sd.at[l, p, kind], rd.at[l, p, kind], partner))

    def handed(l, kinds=(0, 1, 2, 3, 4)):
        for kind in kinds:
            step, half = ((0, None), (1, None), (-1, None), (2, 0), (2, 1))[kind]
            for p in range(3):
                at = held(p, 2, wrap(me[ORDERS[p][2]] - step, 4))
                part = region(l, 1, p, at, 1 - c, half)
                remote(part, part, sd.at[l, p, kind], rd.at[l, p, kind], partner).wait_recv()

    def first3(l):
        for kind in (0, 1):
            for copy, _ in rings3[l]:
                go(copy(kind))

    def second3(l):
        for kind in (2, 3):
            for copy, _ in rings3[l]:
                go(copy(kind))
        for p in range(3):
            hand(l, p, 0)

    def forward3(l):
        for kind in (0, 1):
            for copy, arrived in rings3[l]:
                arrived(kind)
                go(copy(kind + 4))

    def planes3(l):
        for kind in (2, 3):
            for p, (_, arrived) in enumerate(rings3[l]):
                arrived(kind)
                hand(l, p, kind - 1)

    def finish3(l):
        for kind in (4, 5):
            for p, (_, arrived) in enumerate(rings3[l]):
                arrived(kind)
                hand(l, p, kind - 1)

    def parameters():
        for k in range(3):
            part = T.at[wrap(x - (k + 1), 4), share]
            remote(part, part, sp_.at[0, k], rp_.at[0, k], x_peers[k]).wait_recv()
            go(remote(part, part, sp_.at[1, k], rp_.at[1, k], partner))

    def parameters_here():
        for k in range(3):
            part = T.at[wrap(x - (k + 1), 4), pl.ds(17 - 17 * c, 17)]
            remote(part, part, sp_.at[1, k], rp_.at[1, k], partner).wait_recv()

    def halo_across():
        handed(0, (0,))
        go(remote(core_rows, far, sh.at[1], rh.at[1], across))

    def halo_here():
        remote(core_rows, far, sh.at[0], rh.at[0], partner).wait_recv()
        remote(core_rows, near, sh.at[1], rh.at[1], across).wait_recv()

    def norm(l):
        low, rows = STEP * l, 192 - 2 * STEP * l
        src = X if l == 0 else Y
        g = gainv[l : l + 1, :]

        for r in range(low, low + rows, NORM_CHUNK):
            at = pl.ds(r, NORM_CHUNK)
            v = src[at, :].astype(F32)
            scaled = v * lax.rsqrt(jnp.mean(v * v, axis=-1, keepdims=True) + EPSILON)
            N[at, :] = (scaled * g).astype(BF16)

    def project(l, p, dst):
        low, rows = STEP * l, 192 - 2 * STEP * l
        w = W[l, p].reshape(1024, 512)
        dst[pl.ds(low, rows), :] = jnp.dot(N[pl.ds(low, rows), :], w, preferred_element_type=F32)

    def gating(l):
        low, rows = STEP * l, 192 - 2 * STEP * l

        for r in range(low, low + rows, CHUNK):
            at = pl.ds(r, CHUNK)
            g = (V[at, :] * jax.nn.sigmoid(G[at, :])).astype(BF16).astype(F32)
            if r < 64 or r + CHUNK > 128:
                where = sp * 64 - 64 + r + lax.broadcasted_iota(jnp.int32, (CHUNK, 512), 0)
                g = jnp.where((where >= 0) & (where < 2048), g, 0.0)
            for j in range(4):
                GT[j, at, :] = g[:, 128 * j : 128 * j + 128]

    def conv(l):
        low, rows = STEP * (l + 1), 192 - 2 * STEP * (l + 1)
        for j in range(4):
            for r in range(low, low + rows, CHUNK):
                acc = jnp.zeros((CHUNK, 128), F32) + T[j, TAPS, l : l + 1, :]
                for k in range(TAPS):
                    acc = acc + GT[j, r + k - 15 : r + k - 15 + CHUNK, :] * T[j, k, l : l + 1, :]
                CV[r : r + CHUNK, 128 * j : 128 * j + 128] = acc

    def channel_norm(l):
        low, rows = STEP * (l + 1), 192 - 2 * STEP * (l + 1)
        g = jnp.concatenate([T[j, TAPS + 1, l : l + 1, :] for j in range(4)], axis=1)
        b = jnp.concatenate([T[j, TAPS + 2, l : l + 1, :] for j in range(4)], axis=1)

        for r in range(low, low + rows, CHUNK):
            at = pl.ds(r, CHUNK)
            v = CV[at, :]
            centered = v - jnp.mean(v, axis=-1, keepdims=True)
            spread = jnp.mean(centered * centered, axis=-1, keepdims=True)
            v = centered * lax.rsqrt(spread + EPSILON) * g + b
            A[at, :] = (v * jax.nn.sigmoid(v)).astype(BF16)

    def output(l):
        low, rows = STEP * (l + 1), 192 - 2 * STEP * (l + 1)
        src = X if l == 0 else Y
        for q in range(4):
            w = W[l, 2, q].reshape(256, 512)
            branch = lax.dot_general(
                A[pl.ds(low, rows), :], w, (((1,), (1,)), ((), ())), preferred_element_type=F32
            )
            lanes = slice(256 * q, 256 * q + 256)
            total = (src[low : low + rows, lanes].astype(F32) + branch).astype(BF16)
            if l + 1 < LAYERS:
                Y[low : low + rows, lanes] = total
            else:
                O[q] = total

    def compute(l, first=0, last=7):
        steps = (
            norm,
            lambda l: project(l, 0, V),
            lambda l: project(l, 1, G),
            gating,
            conv,
            channel_norm,
            output,
        )
        for step in steps[first:last]:
            step(l)

    end_spread(spreads2[0])
    first3(0)
    second3(0)
    halo_across()
    end_spread(spreads2[1])
    first3(1)
    second3(1)
    parameters()
    end_spread(spreads2[2])
    forward3(0)
    first3(2)
    first3(3)
    planes3(0)
    forward3(1)
    second3(2)
    planes3(1)
    finish3(0)
    halo_here()
    norm(0)
    forward3(2)
    second3(3)
    parameters_here()
    handed(0, (1, 2, 3, 4))
    compute(0, 1, 4)
    forward3(3)
    compute(0, 4, 7)
    finish3(1)
    planes3(2)
    handed(1)
    compute(1, 0, 3)
    finish3(2)
    compute(1, 3, 7)
    planes3(3)
    handed(2)
    compute(2, 0, 3)
    finish3(3)
    compute(2, 3, 7)
    norm(3)
    handed(3)
    compute(3, 1, 7)

    mine = pltpu.make_async_copy(O.at[x], out.at[x], loc.at[10])
    mine.start()
    for k, to in enumerate(x_peers):
        go(remote(O.at[to[1]], out.at[x], so.at[k], ro.at[k], to))
    for k in range(3):
        part = out.at[wrap(x - (k + 1), 4)]
        remote(O.at[0], part, so.at[k], ro.at[k], x_peers[k]).wait_recv()
    mine.wait()
    for copy in sends:
        copy.wait_send()


def carry(src, dst, held, inward, outward):
    ins = [pltpu.make_async_copy(src.at[i], held.at[i], inward.at[i]) for i in range(4)]
    outs = [pltpu.make_async_copy(held.at[i], dst.at[i], outward.at[i]) for i in range(4)]
    for copy in ins:
        copy.start()
    for i, copy in enumerate(ins):
        copy.wait()
        outs[i].start()
    for copy in outs:
        copy.wait()


def shards(tokens, norm_gain, val_weight, gate_weight, conv_taps, conv_bias, ln_gain, ln_shift, out_weight):
    any_ = pl.BlockSpec(memory_space=pltpu.HBM)
    dma = pltpu.SemaphoreType.DMA
    vmem = pltpu.VMEM
    result = pl.pallas_call(
        kernel,
        name="conv_stack",
        out_shape=jax.ShapeDtypeStruct(tokens.shape, tokens.dtype),
        in_specs=[any_] * 9,
        out_specs=pl.BlockSpec(memory_space=pl.ANY),
        scratch_shapes=[
            vmem((LAYERS, 3, 4, 4, 2, 32, 512), BF16),
            vmem((192, 1024), BF16),
            vmem((192, 1024), BF16),
            vmem((192, 1024), BF16),
            vmem((192, 512), F32),
            vmem((192, 512), F32),
            vmem((4, 192, 128), F32),
            vmem((192, 512), F32),
            vmem((192, 512), BF16),
            vmem((4, 64, 256), BF16),
            vmem((LAYERS, 1024), F32),
            vmem((4, TAPS + 3, LAYERS, 128), F32),
            dma((11,)),
            dma((2, 3, 3)), dma((2, 3, 3)),
            dma((3, 3, 3)), dma((3, 3, 3)),
            dma((LAYERS, 3, 6)), dma((LAYERS, 3, 6)),
            dma((LAYERS, 3, 5)), dma((LAYERS, 3, 5)),
            dma((3,)), dma((3,)),
            dma((2,)), dma((2,)),
            dma((2, 3)), dma((2, 3)),
            dma((3,)), dma((3,)),
        ],
        compiler_params=pltpu.CompilerParams(
            collective_id=0, has_side_effects=True, vmem_limit_bytes=67043328
        ),
    )(
        tokens, norm_gain, val_weight, gate_weight, conv_taps.transpose(1, 0, 2), conv_bias, ln_gain, ln_shift,
        out_weight.transpose(0, 2, 1),
    )
    return pl.pallas_call(
        carry,
        name="carry",
        out_shape=jax.ShapeDtypeStruct(tokens.shape, tokens.dtype),
        in_specs=[any_],
        out_specs=any_,
        scratch_shapes=[vmem(tokens.shape, tokens.dtype), dma((4,)), dma((4,))],
        compiler_params=pltpu.CompilerParams(vmem_limit_bytes=67043328),
    )(result)


def solution(mesh):
    return jax.shard_map(
        shards,
        mesh=mesh,
        in_specs=(
            P(None, "sp", "tp"),
            P(),
            P(None, "sp", "tp"),
            P(None, "sp", "tp"),
            P(None, None, "tp"),
            P(None, "tp"),
            P(None, "tp"),
            P(None, "tp"),
            P(None, "tp", "sp"),
        ),
        out_specs=P(None, "sp", "tp"),
        check_vma=False,
    )
```

```python
import functools

import jax
import jax.numpy as jnp
from jax import lax
from jax.experimental import pallas as pl
from jax.experimental.pallas import tpu as pltpu
from jax.sharding import PartitionSpec as P

LAYERS = 4
EPSILON = 1e-06
STEP = 16
TAPS = 31
MESH = pl.DeviceIdType.MESH
F32, BF16 = jnp.float32, jnp.bfloat16
ORDERS = (("x", "y", "z"), ("y", "z", "x"), ("z", "x", "y"))
GROUPS1 = ((0, 1), (1, 1), (2, 2))
GROUPS2 = ((0, 1), (1, 1), (2, 2))
CHUNK = 32
NORM_CHUNK = 32


def wrap(v, n):
    return lax.rem(v + n, n)


def kernel(
    tok, gain, val, gate, taps, bias, lng, lnb, outw, out,
    W, X, Y, N, V, G, GT, CV, A, O, gainv, T,
    loc, s1, r1, s2, r2, s3, r3, sd, rd, st, rt, sh, rh, sp_, rp_, so, ro,
):
    sp = lax.axis_index("sp")
    x = lax.axis_index("tp")
    n_sp = 32
    c = lax.rem(sp, 2)
    y = lax.rem(sp // 2, 4)
    z = sp // 8
    me = {"x": x, "y": y, "z": z}

    def device(d, step):
        at = dict(me)
        at[d] = wrap(me[d] + step, 4)
        return ((at["z"] * 4 + at["y"]) * 2 + c, at["x"])

    partner = (sp + 1 - 2 * c, x)
    across = (wrap(sp + 1 - 2 * (1 - c), n_sp), x)
    x_peers = [(sp, wrap(x + k, 4)) for k in (1, 2, 3)]

    barrier = pltpu.get_barrier_semaphore()
    peers = [device(d, step) for d in "xyz" for step in (1, 2, 3)] + [partner]
    for peer in peers:
        pl.semaphore_signal(barrier, inc=1, device_id=peer, device_id_type=MESH)

    cols = lambda i, w: pl.ds(pl.multiple_of(i * w, w), w)
    parts = (val, gate, outw)
    starts = [pltpu.make_async_copy(w, W.at[:, p, z, y, c, :, cols(x, 128)], loc.at[p]) for p, w in enumerate(parts)]
    starts += [
        pltpu.make_async_copy(tok.at[x], X.at[pl.ds(64, 64), cols(x, 256)], loc.at[3]),
        pltpu.make_async_copy(gain, gainv, loc.at[4]),
        pltpu.make_async_copy(taps, T.at[x, pl.ds(0, TAPS)], loc.at[5]),
        pltpu.make_async_copy(bias, T.at[x, TAPS], loc.at[6]),
        pltpu.make_async_copy(lng, T.at[x, TAPS + 1], loc.at[7]),
        pltpu.make_async_copy(lnb, T.at[x, TAPS + 2], loc.at[8]),
    ]
    for copy in starts:
        copy.start()
    for copy in starts:
        copy.wait()
    pl.semaphore_wait(barrier, len(peers))

    sends = []

    def region(first, count, p, at, core, half):
        pick = lambda v: slice(None) if v is None else v
        rows = slice(None) if half is None else pl.ds(16 * half, 16)
        lanes = slice(None) if at["x"] is None else cols(at["x"], 128)
        return W.at[pl.ds(first, count), p, pick(at["z"]), pick(at["y"]), core, rows, lanes]

    def held(p, phase, coordinate):
        at = dict(me)
        for d in ORDERS[p][:phase]:
            at[d] = None
        at[ORDERS[p][phase]] = coordinate
        return at

    def remote(src, dst, ssem, rsem, to):
        return pltpu.make_async_remote_copy(
            src_ref=src, dst_ref=dst, send_sem=ssem, recv_sem=rsem, device_id=to, device_id_type=MESH
        )

    def ring(p, phase, first, count, ssem, rsem):
        d = ORDERS[p][phase]
        mine = me[d]
        kinds = ((1, 0, 1), (-1, 1, 1), (1, 1, 1), (-1, 0, 1), (1, 0, 2), (-1, 1, 2))

        def copy(kind):
            step, half, hops = kinds[kind]
            part = region(first, count, p, held(p, phase, wrap(mine - step * (hops - 1), 4)), c, half)
            return remote(part, part, ssem.at[kind], rsem.at[kind], device(d, step))

        def arrived(kind):
            step, half, hops = kinds[kind]
            part = region(first, count, p, held(p, phase, wrap(mine - step * hops, 4)), c, half)
            remote(part, part, ssem.at[kind], rsem.at[kind], device(d, step)).wait_recv()

        return copy, arrived

    def go(copy):
        copy.start()
        sends.append(copy)

    def spread(p, phase, first, count, ssem, rsem):
        d = ORDERS[p][phase]

        def copy(k):
            part = region(first, count, p, held(p, phase, me[d]), c, None)
            return remote(part, part, ssem.at[k - 1], rsem.at[k - 1], device(d, k))

        def arrived(k):
            part = region(first, count, p, held(p, phase, wrap(me[d] - k, 4)), c, None)
            remote(part, part, ssem.at[k - 1], rsem.at[k - 1], device(d, k)).wait_recv()

        return copy, arrived

    spreads1 = [[spread(p, 0, f, n, s1.at[g, p], r1.at[g, p]) for p in range(3)] for g, (f, n) in enumerate(GROUPS1)]
    spreads2 = [[spread(p, 1, f, n, s2.at[g, p], r2.at[g, p]) for p in range(3)] for g, (f, n) in enumerate(GROUPS2)]
    rings3 = [[ring(p, 2, l, 1, s3.at[l, p], r3.at[l, p]) for p in range(3)] for l in range(LAYERS)]

    def send_spread(spreads):
        for k in (2, 1, 3):
            for copy, _ in spreads:
                go(copy(k))

    def end_spread(spreads):
        for k in (1, 3, 2):
            for _, arrived in spreads:
                arrived(k)

    def send_tokens(k):
        go(remote(tok.at[x_peers[k][1]], X.at[pl.ds(64, 64), cols(x, 256)], st.at[k], rt.at[k], x_peers[k]))

    share = pl.ds(17 * c, 17)

    def send_parameters(k):
        go(remote(T.at[x, share], T.at[x, share], sp_.at[0, k], rp_.at[0, k], x_peers[k]))

    send_spread(spreads1[0])
    send_spread(spreads1[1])
    send_spread(spreads1[2])
    for k in (1, 0, 2):
        send_tokens(k)
    for k in (1, 0, 2):
        send_parameters(k)
    end_spread(spreads1[0])
    send_spread(spreads2[0])
    end_spread(spreads1[1])
    send_spread(spreads2[1])
    end_spread(spreads1[2])
    send_spread(spreads2[2])
    for k in range(3):
        part = X.at[pl.ds(64, 64), cols(wrap(x - (k + 1), 4), 256)]
        remote(part, part, st.at[k], rt.at[k], x_peers[k]).wait_recv()
    core_rows = X.at[pl.ds(64, 64)]
    near = X.at[pl.ds(128 * c, 64)]
    far = X.at[pl.ds(128 - 128 * c, 64)]
    go(remote(core_rows, near, sh.at[0], rh.at[0], partner))

    def hand(l, p, kind):
        step, half = ((0, None), (1, None), (-1, None), (2, 0), (2, 1))[kind]
        at = held(p, 2, wrap(me[ORDERS[p][2]] - step, 4))
        part = region(l, 1, p, at, c, half)
        go(remote(part, part, sd.at[l, p, kind], rd.at[l, p, kind], partner))

    def handed(l, kinds=(0, 1, 2, 3, 4)):
        for kind in kinds:
            step, half = ((0, None), (1, None), (-1, None), (2, 0), (2, 1))[kind]
            for p in range(3):
                at = held(p, 2, wrap(me[ORDERS[p][2]] - step, 4))
                part = region(l, 1, p, at, 1 - c, half)
                remote(part, part, sd.at[l, p, kind], rd.at[l, p, kind], partner).wait_recv()

    def first3(l):
        for kind in (0, 1):
            for copy, _ in rings3[l]:
                go(copy(kind))

    def second3(l):
        for kind in (2, 3):
            for copy, _ in rings3[l]:
                go(copy(kind))
        for p in range(3):
            hand(l, p, 0)

    def forward3(l):
        for kind in (0, 1):
            for copy, arrived in rings3[l]:
                arrived(kind)
                go(copy(kind + 4))

    def planes3(l):
        for kind in (2, 3):
            for p, (_, arrived) in enumerate(rings3[l]):
                arrived(kind)
                hand(l, p, kind - 1)

    def finish3(l):
        for kind in (4, 5):
            for p, (_, arrived) in enumerate(rings3[l]):
                arrived(kind)
                hand(l, p, kind - 1)

    def parameters():
        for k in range(3):
            part = T.at[wrap(x - (k + 1), 4), share]
            remote(part, part, sp_.at[0, k], rp_.at[0, k], x_peers[k]).wait_recv()
            go(remote(part, part, sp_.at[1, k], rp_.at[1, k], partner))

    def parameters_here():
        for k in range(3):
            part = T.at[wrap(x - (k + 1), 4), pl.ds(17 - 17 * c, 17)]
            remote(part, part, sp_.at[1, k], rp_.at[1, k], partner).wait_recv()

    def halo_across():
        handed(0, (0,))
        go(remote(core_rows, far, sh.at[1], rh.at[1], across))

    def halo_here():
        remote(core_rows, far, sh.at[0], rh.at[0], partner).wait_recv()
        remote(core_rows, near, sh.at[1], rh.at[1], across).wait_recv()

    def norm(l):
        low, rows = STEP * l, 192 - 2 * STEP * l
        src = X if l == 0 else Y
        g = gainv[l : l + 1, :]

        for r in range(low, low + rows, NORM_CHUNK):
            at = pl.ds(r, NORM_CHUNK)
            v = src[at, :].astype(F32)
            scaled = v * lax.rsqrt(jnp.mean(v * v, axis=-1, keepdims=True) + EPSILON)
            N[at, :] = (scaled * g).astype(BF16)

    def project(l, p, dst):
        low, rows = STEP * l, 192 - 2 * STEP * l
        w = W[l, p].reshape(1024, 512)
        dst[pl.ds(low, rows), :] = jnp.dot(N[pl.ds(low, rows), :], w, preferred_element_type=F32)

    def gating(l):
        low, rows = STEP * l, 192 - 2 * STEP * l

        for r in range(low, low + rows, CHUNK):
            at = pl.ds(r, CHUNK)
            g = (V[at, :] * jax.nn.sigmoid(G[at, :])).astype(BF16).astype(F32)
            if r < 64 or r + CHUNK > 128:
                where = sp * 64 - 64 + r + lax.broadcasted_iota(jnp.int32, (CHUNK, 512), 0)
                g = jnp.where((where >= 0) & (where < 2048), g, 0.0)
            for j in range(4):
                GT[j, at, :] = g[:, 128 * j : 128 * j + 128]

    def conv(l):
        low, rows = STEP * (l + 1), 192 - 2 * STEP * (l + 1)
        for j in range(4):
            for r in range(low, low + rows, CHUNK):
                acc = jnp.zeros((CHUNK, 128), F32) + T[j, TAPS, l : l + 1, :]
                for k in range(TAPS):
                    acc = acc + GT[j, r + k - 15 : r + k - 15 + CHUNK, :] * T[j, k, l : l + 1, :]
                CV[r : r + CHUNK, 128 * j : 128 * j + 128] = acc

    def channel_norm(l):
        low, rows = STEP * (l + 1), 192 - 2 * STEP * (l + 1)
        g = jnp.concatenate([T[j, TAPS + 1, l : l + 1, :] for j in range(4)], axis=1)
        b = jnp.concatenate([T[j, TAPS + 2, l : l + 1, :] for j in range(4)], axis=1)

        for r in range(low, low + rows, CHUNK):
            at = pl.ds(r, CHUNK)
            v = CV[at, :]
            centered = v - jnp.mean(v, axis=-1, keepdims=True)
            spread = jnp.mean(centered * centered, axis=-1, keepdims=True)
            v = centered * lax.rsqrt(spread + EPSILON) * g + b
            A[at, :] = (v * jax.nn.sigmoid(v)).astype(BF16)

    def output(l):
        low, rows = STEP * (l + 1), 192 - 2 * STEP * (l + 1)
        src = X if l == 0 else Y
        for q in range(4):
            w = W[l, 2, q].reshape(256, 512)
            branch = lax.dot_general(
                A[pl.ds(low, rows), :], w, (((1,), (1,)), ((), ())), preferred_element_type=F32
            )
            lanes = slice(256 * q, 256 * q + 256)
            total = (src[low : low + rows, lanes].astype(F32) + branch).astype(BF16)
            if l + 1 < LAYERS:
                Y[low : low + rows, lanes] = total
            else:
                O[q] = total

    def compute(l, first=0, last=7):
        steps = (
            norm,
            lambda l: project(l, 0, V),
            lambda l: project(l, 1, G),
            gating,
            conv,
            channel_norm,
            output,
        )
        for step in steps[first:last]:
            step(l)

    end_spread(spreads2[0])
    first3(0)
    second3(0)
    halo_across()
    end_spread(spreads2[1])
    first3(1)
    second3(1)
    parameters()
    end_spread(spreads2[2])
    forward3(0)
    first3(2)
    first3(3)
    planes3(0)
    forward3(1)
    second3(2)
    planes3(1)
    finish3(0)
    halo_here()
    norm(0)
    forward3(2)
    second3(3)
    parameters_here()
    handed(0, (1, 2, 3, 4))
    compute(0, 1, 4)
    forward3(3)
    compute(0, 4, 7)
    finish3(1)
    planes3(2)
    handed(1)
    compute(1, 0, 3)
    finish3(2)
    compute(1, 3, 7)
    planes3(3)
    handed(2)
    compute(2, 0, 3)
    finish3(3)
    compute(2, 3, 7)
    norm(3)
    handed(3)
    compute(3, 1, 7)

    mine = pltpu.make_async_copy(O.at[x], out.at[x], loc.at[10])
    mine.start()
    for k, to in enumerate(x_peers):
        go(remote(O.at[to[1]], out.at[x], so.at[k], ro.at[k], to))
    for k in range(3):
        part = out.at[wrap(x - (k + 1), 4)]
        remote(O.at[0], part, so.at[k], ro.at[k], x_peers[k]).wait_recv()
    mine.wait()
    for copy in sends:
        copy.wait_send()


def shards(tokens, norm_gain, val_weight, gate_weight, conv_taps, conv_bias, ln_gain, ln_shift, out_weight):
    any_ = pl.BlockSpec(memory_space=pltpu.HBM)
    dma = pltpu.SemaphoreType.DMA
    vmem = pltpu.VMEM
    return pl.pallas_call(
        kernel,
        name="conv_stack",
        out_shape=jax.ShapeDtypeStruct(tokens.shape, tokens.dtype),
        in_specs=[any_] * 9,
        out_specs=pl.BlockSpec(memory_space=pl.ANY),
        scratch_shapes=[
            vmem((LAYERS, 3, 4, 4, 2, 32, 512), BF16),
            vmem((192, 1024), BF16),
            vmem((192, 1024), BF16),
            vmem((192, 1024), BF16),
            vmem((192, 512), F32),
            vmem((192, 512), F32),
            vmem((4, 192, 128), F32),
            vmem((192, 512), F32),
            vmem((192, 512), BF16),
            vmem((4, 64, 256), BF16),
            vmem((LAYERS, 1024), F32),
            vmem((4, TAPS + 3, LAYERS, 128), F32),
            dma((11,)),
            dma((3, 3, 3)), dma((3, 3, 3)),
            dma((3, 3, 3)), dma((3, 3, 3)),
            dma((LAYERS, 3, 6)), dma((LAYERS, 3, 6)),
            dma((LAYERS, 3, 5)), dma((LAYERS, 3, 5)),
            dma((3,)), dma((3,)),
            dma((2,)), dma((2,)),
            dma((2, 3)), dma((2, 3)),
            dma((3,)), dma((3,)),
        ],
        compiler_params=pltpu.CompilerParams(
            collective_id=0, has_side_effects=True, vmem_limit_bytes=67043328
        ),
    )(
        tokens, norm_gain, val_weight, gate_weight, conv_taps.transpose(1, 0, 2), conv_bias, ln_gain, ln_shift,
        out_weight.transpose(0, 2, 1),
    )


def solution(mesh):
    return jax.shard_map(
        shards,
        mesh=mesh,
        in_specs=(
            P(None, "sp", "tp"),
            P(),
            P(None, "sp", "tp"),
            P(None, "sp", "tp"),
            P(None, None, "tp"),
            P(None, "tp"),
            P(None, "tp"),
            P(None, "tp"),
            P(None, "tp", "sp"),
        ),
        out_specs=P(None, "sp", "tp"),
        check_vma=False,
    )
```
